32 devices in a mesh: sp: 8 (over z, y), tp: 4 (over x, core).
Axes of the slice: x: 2, y: 2, z: 4, core: 2. Of those that a mesh axis runs over, the one named last changes fastest.
Arguments:
- stream: bfloat16 [3072, 2048], P(('sp', 'tp')), may hold values from -6 to 6
- query_projected: bfloat16 [3072, 1024], P('sp', 'tp'), may hold values from -6 to 6
- key_projected: bfloat16 [3072, 1024], P('sp', 'tp'), may hold values from -6 to 6
- value_projected: bfloat16 [3072, 1024], P('sp', 'tp'), may hold values from -6 to 6
- gate_projected: bfloat16 [3072, 1024], P('sp', 'tp'), may hold values from -6 to 6
- strength_logits: bfloat16 [8, 3072], P('tp', 'sp'), may hold values from -7 to 4
- decay_preactivation: bfloat16 [8, 3072], P('tp', 'sp'), may hold values from -9 to 9
- extra_log_decay: float32 [8, 3072], P('tp', 'sp'), may hold values from -0.7 to 0
- head_decay_rate: float32 [8], P('tp'), may hold values from 0 to 0.1
- head_norm_gain: float32 [128], replicated, may hold values from 0.1 to 1.9
- head_output_matrix: bfloat16 [1024, 2048], P('tp'), may hold values from -0.1875 to 0.1875
- feed_norm_gain: float32 [2048], replicated, may hold values from 0.1 to 1.9
- gate_matrix: bfloat16 [2048, 5632], P('sp', 'tp'), may hold values from -0.125 to 0.125
- up_matrix: bfloat16 [2048, 5632], P('sp', 'tp'), may hold values from -0.125 to 0.125
- down_matrix: bfloat16 [5632, 2048], P('tp', 'sp'), may hold values from -0.078125 to 0.078125
Outputs:
- result: bfloat16 [3072, 2048], P(('sp', 'tp'))
The draws below stay inside these ranges and needn't reach their ends.
All inputs are finite; a program needn't handle non-finite values.
Results may differ from the reference program's by a relative error of at most 0.015.
Values may be sent and summed in bfloat16 or wider, within the bound.
A program may use at most 128 MiB of HBM per device.

```python
import math
import jax
import jax.numpy as jnp
from jax import lax

D = 2048
HEADS = 8
HEAD = 128
FF = 5632
BLOCK = 64
TOK_DEV = 384
HK = 1024
TOKENS = 3072
N_TP = 4


def head_ranking(key):
    return jax.random.permutation(jax.random.fold_in(key, 101), HEADS)


def fast_heads(key):
    fast_count = HEADS // 2
    return head_ranking(key) < fast_count


def draw_head_decay_rate(key, part):
    is_fast = fast_heads(key)
    slow_rate = jnp.exp(jax.random.uniform(jax.random.fold_in(key, 102), (HEADS,), jnp.float32, math.log(0.01), math.log(0.3))) / TOKENS
    fast_rate = jnp.exp(jax.random.uniform(jax.random.fold_in(key, 103), (HEADS,), jnp.float32, math.log(0.03), math.log(0.1)))
    return jnp.where(is_fast, fast_rate, slow_rate).astype(jnp.float32)


def draw_strength_logits(key, part):
    is_fast = fast_heads(key)
    fast_part = jnp.clip(jax.random.normal(jax.random.fold_in(key, 401), (HEADS, TOKENS), jnp.float32), -4.0, 4.0)
    faint_part = jax.random.uniform(jax.random.fold_in(key, 402), (HEADS, TOKENS), jnp.float32, -7.0, -5.0)
    return jnp.where(is_fast[:, None], fast_part, faint_part).astype(jnp.bfloat16)


def draw_decay_preactivation(key, part):
    block_total = TOKENS // TOK_DEV
    noise = jnp.clip(jax.random.normal(jax.random.fold_in(key, 201), (HEADS, block_total, TOK_DEV), jnp.float32), -6.0, 6.0)
    offsets = jax.random.uniform(jax.random.fold_in(key, 202), (block_total,), jnp.float32, -1.5, 1.5)
    return (noise + offsets[None, :, None]).reshape(HEADS, TOKENS).astype(jnp.bfloat16)


def draw_extra_log_decay(key, part):
    places = jax.random.randint(jax.random.fold_in(key, 301), (3,), 0, TOKENS)
    levels = jax.random.uniform(jax.random.fold_in(key, 302), (HEADS, 3), jnp.float32, math.log(0.5), math.log(0.8))
    base = jnp.zeros((HEADS, TOKENS), jnp.float32)
    return base.at[:, places].set(levels).astype(jnp.float32)


def steps_of(stream_key, extent, pieces, low, largest):
    def one(dim, blocks):
        heights = jax.random.uniform(jax.random.fold_in(jax.random.fold_in(stream_key, 6), dim), (blocks,), jnp.float32, low / len(pieces), largest / len(pieces))
        return jnp.repeat(jnp.exp(heights), extent[dim] // blocks).reshape((-1,) + (1,) * (len(extent) - dim - 1))

    level = one(*pieces[0])
    for cut in pieces[1:]:
        level = level * one(*cut)
    return level


def bell_draw(own_key, extent, scale, reach, cuts=(), kind=jnp.bfloat16):
    loudness = steps_of(own_key, extent, cuts, -0.22, 0.18) if cuts else 1.0
    values = jax.random.normal(own_key, extent, jnp.float32) * scale * loudness
    return jnp.minimum(jnp.maximum(values, -reach), reach).astype(kind)


def setup_inputs(seed: int = 0) -> dict:
    seeds = jax.random.split(jax.random.key(seed), 16)
    stream = bell_draw(seeds[0], (TOKENS, D), 1.0, 6.0, ((0, 32),))
    query_projected = bell_draw(seeds[1], (TOKENS, HK), 1.0, 6.0, ((0, 8), (1, 4)))
    key_projected = bell_draw(seeds[2], (TOKENS, HK), 1.0, 6.0, ((0, 8), (1, 4)))
    value_projected = bell_draw(seeds[3], (TOKENS, HK), 1.0, 6.0, ((0, 8), (1, 4)))
    gate_projected = bell_draw(seeds[4], (TOKENS, HK), 1.0, 6.0, ((0, 8), (1, 4)))
    strength_logits = draw_strength_logits(jax.random.fold_in(seeds[15], 71), 0)
    decay_preactivation = draw_decay_preactivation(jax.random.fold_in(seeds[15], 71), 0)
    extra_log_decay = draw_extra_log_decay(jax.random.fold_in(seeds[15], 71), 0)
    head_decay_rate = draw_head_decay_rate(jax.random.fold_in(seeds[15], 71), 0)
    head_norm_gain = jnp.clip(1.0 + 0.18 * jax.random.normal(seeds[9], (HEAD,), jnp.float32), 0.1, 1.9)
    head_output_matrix = bell_draw(seeds[10], (HK, D), HK ** -0.5, 0.1875, ((0, 4),))
    feed_norm_gain = jnp.clip(1.0 + 0.18 * jax.random.normal(seeds[11], (D,), jnp.float32), 0.1, 1.9)
    gate_matrix = bell_draw(seeds[12], (D, FF), D ** -0.5, 0.125, ((0, 8), (1, 4)))
    up_matrix = bell_draw(seeds[13], (D, FF), D ** -0.5, 0.125, ((0, 8), (1, 4)))
    down_matrix = bell_draw(seeds[14], (FF, D), FF ** -0.5, 0.078125, ((0, 4), (1, 8)))
    return dict(stream=stream, query_projected=query_projected, key_projected=key_projected, value_projected=value_projected, gate_projected=gate_projected, strength_logits=strength_logits, decay_preactivation=decay_preactivation, extra_log_decay=extra_log_decay, head_decay_rate=head_decay_rate, head_norm_gain=head_norm_gain, head_output_matrix=head_output_matrix, feed_norm_gain=feed_norm_gain, gate_matrix=gate_matrix, up_matrix=up_matrix, down_matrix=down_matrix)


PRECISION_FULL = lax.Precision.HIGHEST
EPSILON = 1e-06

def unit_rows(tensor):
    return tensor * lax.rsqrt(lax.optimization_barrier(jnp.sum(tensor * tensor, axis=-1, keepdims=True)) + EPSILON)

def block_correction(unit_queries, unit_keys, complete_values, strength_logits, decay_preactivation, extra_log_decay, head_decay_rate):
    head_count, length, head_width = unit_queries.shape
    block_count = length // BLOCK

    def to_blocks(tensor):
        return tensor.reshape((head_count, block_count, BLOCK) + tensor.shape[2:])
    beta_gate = jax.nn.sigmoid(strength_logits.astype(jnp.float32))
    decay_logarithm = -head_decay_rate[:, None] * jax.nn.softplus(decay_preactivation.astype(jnp.float32)) + extra_log_decay
    query_block = to_blocks(unit_queries)
    key_block = to_blocks(unit_keys)
    value_block = to_blocks(complete_values)
    beta_block = to_blocks(beta_gate)
    cumulative = jnp.cumsum(to_blocks(decay_logarithm), axis=-1)
    causal = jnp.tril(jnp.ones((BLOCK, BLOCK), bool))
    strict = jnp.tril(jnp.ones((BLOCK, BLOCK), bool), -1)
    spread = cumulative[..., :, None] - cumulative[..., None, :]
    damping = jnp.where(causal, jnp.exp(jnp.where(causal, spread, 0.0)), 0.0)
    key_beta = key_block * beta_block[..., None]
    lower_part = jnp.einsum('hnid,hnjd->hnij', key_beta, key_block, precision=PRECISION_FULL) * jnp.where(strict, damping, 0.0)
    system = lower_part + jnp.eye(BLOCK, dtype=jnp.float32)
    right_side = jnp.concatenate([value_block * beta_block[..., None], key_beta * jnp.exp(cumulative)[..., None]], axis=-1)
    solved = lax.linalg.triangular_solve(system, right_side, left_side=True, lower=True, unit_diagonal=True)
    target_values = solved[..., :head_width]
    householder_weights = solved[..., head_width:]
    inner_scores = jnp.einsum('hnid,hnjd->hnij', query_block, key_block, precision=PRECISION_FULL) * damping
    decayed_queries = query_block * jnp.exp(cumulative)[..., None]
    closing_log_decay = cumulative[..., -1:]
    decayed_keys = key_block * jnp.exp(closing_log_decay - cumulative)[..., None]
    return (decayed_queries, decayed_keys, target_values, householder_weights, inner_scores, closing_log_decay)

def advance(running_state, items):
    decayed_queries, decayed_keys, target_values, householder_weights, inner_scores, closing_log_decay = items
    new_state = target_values - jnp.einsum('fdc,fcj->fdj', householder_weights, running_state, precision=PRECISION_FULL)
    layer_output = jnp.einsum('fdc,fcj->fdj', decayed_queries, running_state, precision=PRECISION_FULL)
    layer_output = layer_output + jnp.einsum('hij,hjv->hiv', inner_scores, new_state, precision=PRECISION_FULL)
    running_state = jnp.exp(closing_log_decay)[:, :, None] * running_state + jnp.einsum('xwp,xws->xps', decayed_keys, new_state, precision=PRECISION_FULL)
    return (running_state, layer_output)

def split_heads(tensor):
    return tensor.reshape(TOKENS, HEADS, HEAD).transpose(1, 0, 2).astype(jnp.float32)

def rms_scale(tensor):
    return tensor * lax.rsqrt(lax.optimization_barrier(jnp.mean(tensor * tensor, axis=-1, keepdims=True)) + EPSILON)

def reference(stream, query_projected, key_projected, value_projected, gate_projected, strength_logits, decay_preactivation, extra_log_decay, head_decay_rate, head_norm_gain, head_output_matrix, feed_norm_gain, gate_matrix, up_matrix, down_matrix):
    unit_queries = unit_rows(split_heads(query_projected)) * HEAD ** (-0.5)
    unit_keys = unit_rows(split_heads(key_projected))
    complete_values = split_heads(value_projected)
    score_terms = block_correction(unit_queries, unit_keys, complete_values, strength_logits, decay_preactivation, extra_log_decay, head_decay_rate)
    moved = tuple((jnp.moveaxis(tensor, 1, 0) for tensor in score_terms))
    initial = jnp.zeros((HEADS, HEAD, HEAD), jnp.float32)
    _, block_outputs = lax.scan(advance, initial, moved)
    attention_output = jnp.moveaxis(block_outputs, 0, 1).reshape(HEADS, TOKENS, HEAD)
    normed_heads = rms_scale(attention_output) * head_norm_gain
    gated = normed_heads.transpose(1, 0, 2).reshape(TOKENS, HK) * jax.nn.silu(gate_projected.astype(jnp.float32))
    mixed = gated.astype(jnp.bfloat16)
    group_width = HK // N_TP
    branch = jnp.zeros((TOKENS, D), jnp.float32)
    for group in range(N_TP):
        piece = jnp.dot(mixed[:, group * group_width:(group + 1) * group_width].astype(jnp.float32), head_output_matrix[group * group_width:(group + 1) * group_width].astype(jnp.float32), preferred_element_type=jnp.float32)
        branch = branch + piece.astype(jnp.bfloat16).astype(jnp.float32)
    residual = stream.astype(jnp.float32) + branch
    normed = (rms_scale(residual) * feed_norm_gain).astype(jnp.bfloat16)
    gate = jnp.dot(normed.astype(jnp.float32), gate_matrix.astype(jnp.float32), preferred_element_type=jnp.float32)
    up_value = jnp.dot(normed.astype(jnp.float32), up_matrix.astype(jnp.float32), preferred_element_type=jnp.float32)
    hidden = (jax.nn.silu(gate) * up_value).astype(jnp.bfloat16)
    unit_group = FF // N_TP
    ffn_total = jnp.zeros((TOKENS, D), jnp.float32)
    for group in range(N_TP):
        piece = jnp.dot(hidden[:, group * unit_group:(group + 1) * unit_group].astype(jnp.float32), down_matrix[group * unit_group:(group + 1) * unit_group].astype(jnp.float32), preferred_element_type=jnp.float32)
        ffn_total = ffn_total + piece.astype(jnp.bfloat16).astype(jnp.float32)
    return (residual + ffn_total).astype(jnp.bfloat16)
```

```python
import functools

import jax
import jax.numpy as jnp
from jax import lax
from jax.experimental import pallas as pl
from jax.experimental.pallas import tpu as pltpu
from jax.sharding import PartitionSpec as P

HEAD = 128
CHUNK = 128
UNROLLED = 8
EPSILON = 1e-06
F32 = jnp.float32
BF16 = jnp.bfloat16
HIGHEST = lax.Precision.HIGHEST
NN = (((1,), (0,)), ((), ()))
NT = (((1,), (1,)), ((), ()))
TN = (((0,), (0,)), ((), ()))


def dot1(a, b, dims=NN):
    return lax.dot_general(a, b, dims, preferred_element_type=F32)


def halves(x):
    high = x.astype(BF16)
    return high, (x - high.astype(F32)).astype(BF16)


def dot3(a, b, dims=NN):
    ah, al = halves(a)
    bh, bl = halves(b)
    return dot1(ah, bh, dims) + (dot1(ah, bl, dims) + dot1(al, bh, dims))


def silu(x):
    return x * jax.nn.sigmoid(x)


def local_scan(qp, kp, vp, strength, decay_pre, extra, rate, out_scr):
    heads, tokens = strength.shape
    chunks = tokens // CHUNK
    row_i = lax.broadcasted_iota(jnp.int32, (CHUNK, CHUNK), 0)
    col_i = lax.broadcasted_iota(jnp.int32, (CHUNK, CHUNK), 1)
    causal = row_i >= col_i
    strict = row_i > col_i
    eye = jnp.where(row_i == col_i, 1.0, 0.0).astype(F32)
    lower = jnp.where(causal, 1.0, 0.0).astype(F32)
    beta = jax.nn.sigmoid(strength[...].astype(F32))
    pre = decay_pre[...].astype(F32)
    soft = jnp.maximum(pre, 0.0) + jnp.log1p(jnp.exp(-jnp.abs(pre)))
    log_decay = -rate[...] * soft + extra[...]

    pairs = [(h, c) for c in range(chunks) for h in range(heads)]
    data = {}
    for c in range(chunks):
        span = slice(c * CHUNK, (c + 1) * CHUNK)
        ld = log_decay[:, span]
        c_row = lax.dot_general(ld, lower, NT, precision=HIGHEST, preferred_element_type=F32)
        c_col = lax.dot_general(lower, ld, NT, precision=HIGHEST, preferred_element_type=F32)
        b_col = lax.dot_general(eye, beta[:, span], NT, precision=HIGHEST, preferred_element_type=F32)
        for h in range(heads):
            lanes = slice(h * HEAD, (h + 1) * HEAD)
            q = qp[span, lanes].astype(F32)
            k = kp[span, lanes].astype(F32)
            v = vp[span, lanes].astype(F32)
            q = q * (lax.rsqrt(jnp.sum(q * q, axis=-1, keepdims=True) + EPSILON) * HEAD ** (-0.5))
            k = k * lax.rsqrt(jnp.sum(k * k, axis=-1, keepdims=True) + EPSILON)
            cc = c_col[:, h:h + 1]
            bb = b_col[:, h:h + 1]
            cr = c_row[h:h + 1, :]
            last = cr[:, CHUNK - 1:]
            damp = jnp.where(causal, jnp.exp(jnp.where(causal, cc - cr, 0.0)), 0.0)
            grown = jnp.exp(cc)
            kb = k * bb
            kk = dot3(kb, k, NT) * jnp.where(strict, damp, 0.0)
            inner = dot3(q, k, NT) * damp
            data[h, c] = dict(
                low=kk, inner=inner, v=v * bb, kw=kb * grown, qd=q * grown,
                kd=k * jnp.exp(last - cc), decay=jnp.exp(last),
            )
    inverse = {}
    b = 1
    shift = 0
    while b < CHUNK:
        mask = ((row_i >> (shift + 1)) == (col_i >> (shift + 1))) & (
            ((row_i >> shift) & 1) == 1) & (((col_i >> shift) & 1) == 0)
        for key in pairs:
            piece = jnp.where(mask, data[key]["low"], 0.0)
            if b == 1:
                inverse[key] = eye - piece
            else:
                x = inverse[key]
                inverse[key] = x - dot3(x, dot3(piece, x))
        b *= 2
        shift += 1
    states = [jnp.concatenate([jnp.zeros((HEAD, HEAD), F32), eye], axis=1) for _ in range(heads)]
    for c in range(chunks):
        for h in range(heads):
            e = data[h, c]
            u = dot3(inverse[h, c], e["v"])
            w = dot3(inverse[h, c], e["kw"])
            x = states[h]
            new = jnp.concatenate([u, jnp.zeros_like(u)], axis=1) - dot3(w, x)
            out_scr[h, c * CHUNK:(c + 1) * CHUNK, :] = dot3(e["qd"], x) + dot3(e["inner"], new)
            states[h] = e["decay"] * x + dot3(e["kd"], new, TN)
    return states


def combine(states, x_part, p, p_send):
    heads = len(states)
    for h in range(heads):
        mine = states[h]
        theirs = x_part[h].astype(F32)
        before = jnp.where(p == 0, mine, theirs)
        after = jnp.where(p == 0, theirs, mine)
        after_s = jnp.concatenate([after[:, :HEAD], jnp.zeros((HEAD, HEAD), F32)], axis=1)
        p_send[h] = (dot3(after[:, HEAD:], before) + after_s).astype(BF16)


def fold_states(r, p_recv, s_in, heads):
    s_in[...] = jnp.zeros_like(s_in)

    def fold(i, _):
        for h in range(heads):
            got = p_recv[i, h].astype(F32)
            s_in[h] = dot3(got[:, HEAD:], s_in[h]) + got[:, :HEAD]
        return 0

    lax.fori_loop(0, r, fold, 0)


def apply_state(p, x_part, s_in, out_scr, head_gain, gp, mixed, heads):
    for h in range(heads):
        lanes = slice(h * HEAD, (h + 1) * HEAD)
        got = x_part[h].astype(F32)
        s = s_in[h]
        s = jnp.where(p == 0, s, dot3(got[:, HEAD:], s) + got[:, :HEAD])
        att = out_scr[h, :, :HEAD] + dot3(out_scr[h, :, HEAD:], s)
        att = att * lax.rsqrt(jnp.mean(att * att, axis=-1, keepdims=True) + EPSILON) * head_gain[...]
        mixed[:, lanes] = (att * silu(gp[:, lanes].astype(F32))).astype(BF16)


def messages(ring):
    own_z = [(a, 0, 0, way) for a in "GU" for way in "RL"]
    own_y = [(a, 0, 0, "Y") for a in "GU"]
    first = own_z + own_y
    down_y = [("D", 0, 0, "Y")]

    def relay(a, j, skip_y=False):
        out = []
        if j < ring - 1:
            out += [(a, -j, 0, "R"), (a, j, 0, "L")]
        if not skip_y:
            out += [(a, -j, 0, "Y"), (a, j, 0, "Y")]
        return out

    early, middle, later, last = [], [], [], []
    if ring > 1:
        early = relay("G", 1)
        middle = relay("U", 1)
        for j in range(2, ring):
            later += relay("G", j) + relay("U", j)
            if j == 2:
                later += [("D", 0, 0, "R"), ("D", 0, 0, "L")]
        if ring == 2:
            later += [("D", 0, 0, "R"), ("D", 0, 0, "L")]
        later += [("D", 0, 1, "R"), ("D", 0, 1, "L")]
        later += relay("D", 1, skip_y=True)
        for j in range(2, ring):
            last += relay("D", j)
    else:
        first = own_y
    return first, down_y, early, middle, later, last


def chain_kernel(
    n, tps, groups,
    stream, qp, kp, vp, gp, strength, decay_pre, extra, rate, head_gain, w_out, feed_gain,
    gate_in, up_in, down_in,
    result,
    gate_all, up_all, down_all, out_scr, x_send, x_part, p_send, p_recv, s_in, mixed,
    d_send, d_recv, residual, rows_all, hidden, f_part, f_recv,
    w_send, w_recv, own_sem, x_sem, p_ssem, p_rsem, d_ssem, d_rsem, e_ssem, e_rsem, f_ssem, f_rsem,
):
    ring = n // 2
    sp = lax.axis_index("sp")
    tp = lax.axis_index("tp")
    r = sp // 2
    p = lax.rem(sp, 2)
    heads = strength.shape[0]
    tokens = strength.shape[1]
    chunks = tokens // CHUNK
    own_rows = stream.shape[0]
    kr = gate_in.shape[0]
    MESH = pl.DeviceIdType.MESH

    def sp_of(dr, rel):
        q = p if rel == 0 else 1 - p
        return lax.rem(r + dr + ring, ring) * 2 + q

    partner = sp_of(0, 1)
    where = {"R": sp_of(1, 0), "L": sp_of(-1, 0), "Y": partner}

    def tp_peer(o):
        return lax.rem(tp + o, tps)

    barrier = pltpu.get_barrier_semaphore()
    for dr in range(1, ring):
        pl.semaphore_signal(barrier, 1, device_id=(sp_of(dr, 0), tp), device_id_type=MESH)
    pl.semaphore_signal(barrier, 1, device_id=(partner, tp), device_id_type=MESH)
    for o in range(1, tps):
        pl.semaphore_signal(barrier, 1, device_id=(sp, tp_peer(o)), device_id_type=MESH)
    pl.semaphore_wait(barrier, ring + tps - 1)

    flat = [m for g in groups for m in g]
    number = {m: i for i, m in enumerate(flat)}
    arrival = {}
    for (a, dr, rel, way) in flat:
        to = {"R": (dr - 1, rel), "L": (dr + 1, rel), "Y": (dr, 1 - rel)}[way]
        key = (a, to[0], to[1])
        assert key not in arrival
        arrival[key] = number[(a, dr, rel, way)]
    waited = set()
    copies = []

    def exists(dr):
        return (r + dr >= 0) & (r + dr < ring)

    def slot(a, dr, rel):
        s = sp_of(dr, rel)
        if a == "D":
            return down_all.at[s]
        whole = gate_all if a == "G" else up_all
        return whole.at[pl.ds(pl.multiple_of(s * kr, kr), kr), :]

    inputs = {"G": gate_in, "U": up_in, "D": down_in}

    def need(a, dr, rel):
        key = (a, dr, rel)
        if (dr == 0 and rel == 0) or key in waited:
            return
        waited.add(key)
        m = arrival[key]

        @pl.when(exists(dr))
        def _():
            here = slot(*key)
            pltpu.make_async_remote_copy(
                here, here, w_send.at[m], w_recv.at[m], device_id=(partner, tp), device_id_type=MESH
            ).wait_recv()

    def outgoing(message):
        a, dr, rel, way = message
        m = number[message]
        return pltpu.make_async_remote_copy(
            inputs[a] if dr == 0 and rel == 0 else slot(a, dr, rel),
            slot(a, dr, rel),
            w_send.at[m], w_recv.at[m],
            device_id=(where[way], tp), device_id_type=MESH,
        )

    def goes(message):
        ahead = {"R": r + 1 < ring, "L": r >= 1, "Y": r >= 0}[message[3]]
        return exists(message[1]) & ahead

    def pump(group):
        for message in group:
            need(*message[:3])

            @pl.when(goes(message))
            def _():
                outgoing(message).start()

            copies.append(message)

    def need_all(a):
        for dr in sorted(range(1 - ring, ring), key=abs):
            for rel in (0, 1):
                need(a, dr, rel)

    first, down_y, early, middle, later, last_group = groups
    pump(first)
    locals_ = []
    for i, a in enumerate("GUD"):
        local = pltpu.make_async_copy(inputs[a], slot(a, 0, 0), own_sem.at[i])
        local.start()
        locals_.append(local)

    states = local_scan(qp, kp, vp, strength, decay_pre, extra, rate, out_scr)
    for h in range(heads):
        x_send[h] = states[h].astype(BF16)
    x_copy = pltpu.make_async_remote_copy(
        x_send, x_part, x_sem.at[0], x_sem.at[1], device_id=(partner, tp), device_id_type=MESH)
    x_copy.start()
    pump(down_y)
    x_copy.wait_recv()
    combine(states, x_part, p, p_send)

    def p_copy(k, to, at):
        return pltpu.make_async_remote_copy(
            p_send, p_recv.at[at], p_ssem.at[k], p_rsem.at[k],
            device_id=(to, tp), device_id_type=MESH)

    for k in range(1, ring):
        @pl.when(r + k < ring)
        def _():
            p_copy(k, sp_of(k, 0), r).start()
    pump(early)
    for k in range(1, ring):
        @pl.when(r - k >= 0)
        def _():
            p_copy(k, sp_of(-k, 0), r - k).wait_recv()
    fold_states(r, p_recv, s_in, heads)
    apply_state(p, x_part, s_in, out_scr, head_gain, gp, mixed, heads)

    def rows_of(t):
        return pl.ds(pl.multiple_of(t * own_rows, own_rows), own_rows)

    order = [o for o in (2, 3, 1) if o < tps] + list(range(4, tps))
    d_copies = []
    for o in order:
        to = tp_peer(o)
        d_send[o - 1] = dot1(mixed[rows_of(to), :], w_out[...]).astype(BF16)
        copy = pltpu.make_async_remote_copy(
            d_send.at[o - 1], d_recv.at[o - 1], d_ssem.at[o - 1], d_rsem.at[o - 1],
            device_id=(sp, to), device_id_type=MESH)
        copy.start()
        d_copies.append(copy)
    pump(middle)
    total = dot1(mixed[rows_of(tp), :], w_out[...]).astype(BF16).astype(F32)
    for copy in d_copies:
        copy.wait_recv()
    for o in range(1, tps):
        total = total + d_recv[o - 1].astype(F32)
    total = stream[...].astype(F32) + total
    residual[...] = total
    rows_all[rows_of(tp), :] = (
        total * lax.rsqrt(jnp.mean(total * total, axis=-1, keepdims=True) + EPSILON) * feed_gain[...]
    ).astype(BF16)
    e_copies = []
    for o in order:
        copy = pltpu.make_async_remote_copy(
            rows_all.at[rows_of(tp), :], rows_all.at[rows_of(tp), :], e_ssem.at[o - 1], e_rsem.at[o - 1],
            device_id=(sp, tp_peer(o)), device_id_type=MESH)
        copy.start()
        e_copies.append(copy)
    for o in order:
        there = rows_all.at[rows_of(lax.rem(tp - o + tps, tps)), :]
        pltpu.make_async_remote_copy(
            there, there, e_ssem.at[o - 1], e_rsem.at[o - 1],
            device_id=(sp, tp_peer(o)), device_id_type=MESH).wait_recv()
    pump(later)
    need_all("G")
    need_all("U")
    for local in locals_:
        local.wait()

    tile = 128

    def ffn_in(i, _):
        lanes = pl.ds(pl.multiple_of(i * tile, tile), tile)
        both = dot1(rows_all[...], jnp.concatenate([gate_all[:, lanes], up_all[:, lanes]], axis=1))
        hidden[:, lanes] = (silu(both[:, :tile]) * both[:, tile:]).astype(BF16)
        return 0

    lax.fori_loop(0, gate_all.shape[1] // tile, ffn_in, 0)
    pump(last_group)
    need_all("D")
    dc = down_all.shape[2]
    pack = max(1, 128 // dc)
    wide = pack * dc

    def ffn_out(i, _):
        lanes = pl.ds(pl.multiple_of(i * wide, wide), wide)
        if pack == 1:
            weights = down_all[i]
        else:
            weights = jnp.concatenate([down_all[i * pack + j] for j in range(pack)], axis=1)
        f_part[:, lanes] = dot1(hidden[...], weights).astype(BF16)
        return 0

    lax.fori_loop(0, n // pack, ffn_out, 0)
    f_copies = []
    for o in order:
        copy = pltpu.make_async_remote_copy(
            f_part.at[rows_of(tp_peer(o)), :], f_recv.at[o - 1], f_ssem.at[o - 1], f_rsem.at[o - 1],
            device_id=(sp, tp_peer(o)), device_id_type=MESH)
        copy.start()
        f_copies.append(copy)
    ffn = f_part[rows_of(tp), :].astype(F32)
    for copy in f_copies:
        copy.wait_recv()
    for o in range(1, tps):
        ffn = ffn + f_recv[o - 1].astype(F32)
    result[...] = (residual[...] + ffn).astype(BF16)

    for message in copies:
        @pl.when(goes(message))
        def _():
            outgoing(message).wait_send()
    for copy in [x_copy] + d_copies + e_copies + f_copies:
        copy.wait_send()
    for k in range(1, ring):
        @pl.when(r + k < ring)
        def _():
            p_copy(k, sp_of(k, 0), r).wait_send()


def chain_body(n, tps, stream, qp, kp, vp, gp, strength, decay_pre, extra, rate, head_gain, w_out,
         feed_gain, gate_m, up_m, down_m):
    heads, tokens = strength.shape
    own, width = stream.shape
    kr, units = gate_m.shape
    ring = n // 2
    groups = messages(ring)
    count = sum(len(g) for g in groups)
    dma = pltpu.SemaphoreType.DMA
    vmem = pl.BlockSpec(memory_space=pltpu.VMEM)
    hbm = pl.BlockSpec(memory_space=pl.ANY)
    peers = max(1, tps - 1)
    return pl.pallas_call(
        functools.partial(chain_kernel, n, tps, groups),
        out_shape=jax.ShapeDtypeStruct((own, width), BF16),
        in_specs=[vmem] * 12 + [hbm] * 3,
        out_specs=vmem,
        scratch_shapes=[
            pltpu.VMEM((kr * n, units), BF16),
            pltpu.VMEM((kr * n, units), BF16),
            pltpu.VMEM((n,) + down_m.shape, BF16),
            pltpu.VMEM((heads, tokens, 2 * HEAD), F32),
            pltpu.VMEM((heads, HEAD, 2 * HEAD), BF16),
            pltpu.VMEM((heads, HEAD, 2 * HEAD), BF16),
            pltpu.VMEM((heads, HEAD, 2 * HEAD), BF16),
            pltpu.VMEM((ring, heads, HEAD, 2 * HEAD), BF16),
            pltpu.VMEM((heads, HEAD, HEAD), F32),
            pltpu.VMEM((tokens, heads * HEAD), BF16),
            pltpu.VMEM((peers, own, width), BF16),
            pltpu.VMEM((peers, own, width), BF16),
            pltpu.VMEM((own, width), F32),
            pltpu.VMEM((tokens, width), BF16),
            pltpu.VMEM((tokens, units), BF16),
            pltpu.VMEM((tokens, width), BF16),
            pltpu.VMEM((peers, own, width), BF16),
            dma((count,)), dma((count,)), dma((3,)), dma((2,)), dma((ring,)), dma((ring,)),
            dma((peers,)), dma((peers,)), dma((peers,)), dma((peers,)), dma((peers,)), dma((peers,)),
        ],
        compiler_params=pltpu.CompilerParams(
            collective_id=0, has_side_effects=True, vmem_limit_bytes=60 * 1024 * 1024),
    )(stream, qp, kp, vp, gp, strength, decay_pre, extra, rate[:, None], head_gain[None, :], w_out,
      feed_gain[None, :], gate_m, up_m, down_m)


def regions_of(ring, units):
    tiles = units // 128
    side = (tiles - 1) // 2 * 128
    half, quarter = ring // 2, ring // 4
    return {
        "L": (0, half, 0, side),
        "M": (quarter, half + quarter, side, units - side),
        "H": (half, ring, units - side, units),
    }


def paired_kernel(
    n, tps,
    stream, qp, kp, vp, gp, strength, decay_pre, extra, rate, head_gain, feed_gain,
    w_out, gate_in, up_in, down_in,
    result,
    gate_all, up_all, down_all, w_all, out_scr, x_send, x_part, p_send, p_recv, s_in, mixed, mix_all,
    residual, rows_all, hidden, acc, acc2, acc3, fd_send, fd_recv, fx_send, fx_recv, fz_send, fz_recv,
    w_send, w_recv, own_sem, x_sem, p_ssem, p_rsem, wo_ssem, wo_rsem, m_ssem, m_rsem, t_ssem, t_rsem,
    fd_ssem, fd_rsem, fx_ssem, fx_rsem, fz_ssem, fz_rsem,
):
    ring = n // 2
    half = ring // 2
    sp = lax.axis_index("sp")
    tp = lax.axis_index("tp")
    r = sp // 2
    p = lax.rem(sp, 2)
    x = tp // 2
    c = lax.rem(tp, 2)
    zz = jnp.where(r >= half, 1, 0)
    heads = strength.shape[0]
    own_rows = stream.shape[0]
    kr, units = gate_in.shape
    width = stream.shape[1]
    dc = down_in.shape[1]
    MESH = pl.DeviceIdType.MESH
    regions = regions_of(ring, units)
    partner = r * 2 + 1 - p
    mate = lax.rem(r + half, ring) * 2 + p
    core = x * 2 + 1 - c
    across = (1 - x) * 2 + c
    diagonal = (1 - x) * 2 + 1 - c

    def at(q):
        return q * 2 + p

    def remote(src, dst, ssem, rsem, sp_to, tp_to):
        return pltpu.make_async_remote_copy(src, dst, ssem, rsem, device_id=(sp_to, tp_to), device_id_type=MESH)

    inputs = {"G": gate_in, "U": up_in, "D": down_in}
    keys = [(a, g, q, rel) for a in "GUD" for g in "LMH" for q in range(ring) for rel in (0, 1)]
    number = {key: i for i, key in enumerate(keys)}

    def slot(a, g, q, rel):
        s = q * 2 + (p if rel == 0 else 1 - p)
        c0, c1 = regions[g][2:]
        if a == "D":
            return down_all.at[s, c0:c1, :]
        whole = gate_all if a == "G" else up_all
        return whole.at[pl.ds(pl.multiple_of(s * kr, kr), kr), c0:c1]

    def own(a, g):
        c0, c1 = regions[g][2:]
        return inputs[a].at[c0:c1, :] if a == "D" else inputs[a].at[:, c0:c1]

    def member(g):
        return (r >= regions[g][0]) & (r < regions[g][1])

    own_copies = []
    for i, a in enumerate("GUD"):
        for j, g in enumerate("LMH"):
            for q in range(*regions[g][:2]):
                copy = pltpu.make_async_copy(own(a, g), slot(a, g, q, 0), own_sem.at[3 * i + j])
                own_copies.append((r == q, copy))

                @pl.when(r == q)
                def _():
                    copy.start()

    w_local = pltpu.make_async_copy(w_out, w_all.at[tp], own_sem.at[9])
    w_local.start()

    barrier = pltpu.get_barrier_semaphore()
    for k in range(1, ring):
        pl.semaphore_signal(barrier, 1, device_id=(at(lax.rem(r + k, ring)), tp), device_id_type=MESH)
    pl.semaphore_signal(barrier, 1, device_id=(partner, tp), device_id_type=MESH)
    for k in range(1, tps):
        pl.semaphore_signal(barrier, 1, device_id=(sp, lax.rem(tp + k, tps)), device_id_type=MESH)
    pl.semaphore_wait(barrier, ring + tps - 1)

    def detour(a, g, q, to):
        lo, hi = regions[g][:2]
        if g == "M" or hi - lo < 2:
            return False
        inner, outer = (hi - 1, hi - 2) if g == "L" else (lo, lo + 1)
        return (q, to) == (outer, inner) or (a == "D" and (q, to) == (inner, outer))

    sends = []
    waited = set()

    def send(cond, src, key, way, sp_to):
        m = number[key]
        dst = slot(key[0], key[1], key[2], key[3] if way != 3 else 0)

        def make():
            return remote(src, dst, w_send.at[m, way], w_recv.at[number[key[:3] + (1 if way == 3 else key[3],)]], sp_to, tp)

        @pl.when(cond)
        def _():
            make().start()

        sends.append((cond, make))

    def y_cond(a, g, q, base):
        cond = base
        lo, hi = regions[g][:2]
        for to in range(lo, hi):
            if detour(a, g, q, to):
                cond = cond & (r != to)
        return cond

    def own_sends(a, ways):
        for g in "LMH":
            lo, hi = regions[g][:2]
            for q in range(ring):
                key = (a, g, q, 0)
                mine = r == q
                if lo <= q < hi:
                    here = slot(*key)
                    if "l" in ways and q > lo:
                        send(mine, here, key, 0, at(q - 1))
                    if "r" in ways and q + 1 < hi:
                        send(mine, here, key, 1, at(q + 1))
                    if "y" in ways:
                        send(mine, here, key, 3, partner)
                elif "r" in ways and q < lo:
                    send(mine, own(a, g), key, 2, at(lo))
                elif "l" in ways and q >= hi:
                    send(mine, own(a, g), key, 2, at(hi - 1))

    def need(key):
        if key in waited:
            return
        waited.add(key)
        a, g, q, rel = key
        cond = member(g)
        if rel == 0:
            cond = cond & (r != q)

        @pl.when(cond)
        def _():
            here = slot(*key)
            m = number[key]
            remote(here, here, w_send.at[m, 0], w_recv.at[m], partner, tp).wait_recv()

    def relay(a, g, q):
        key = (a, g, q, 0)
        lo, hi = regions[g][:2]
        need(key)
        here = slot(*key)
        if min(q - 1, hi - 1) >= lo + 1:
            send((r > lo) & (r < min(q, hi)), here, key, 0, at(r - 1))
        if max(q + 1, lo) <= hi - 2:
            send((r >= max(q + 1, lo)) & (r < hi - 1), here, key, 1, at(r + 1))
        send(y_cond(a, g, q, member(g) & (r != q)), here, key, 3, partner)

    def detours(a):
        for g in "LH":
            for q in range(*regions[g][:2]):
                for to, way in ((q - 1, 0), (q + 1, 1)):
                    if detour(a, g, q, to):
                        key = (a, g, q, 1)
                        m = number[key]
                        here = slot(*key)
                        cond = r == q

                        @pl.when(cond)
                        def _():
                            remote(here, here, w_send.at[m, 0], w_recv.at[m], partner, tp).wait_recv()

                        early.setdefault(key, []).append(q)
                        send(cond, here, key, way, at(to))

    early = {}
    low = list(range(half - 1, -1, -1)) + list(range(half, ring))
    high = [ring - 1 - q for q in low]
    middle = sorted(range(ring), key=lambda q: abs(2 * q - ring + 1))

    def relays(a, part):
        cut = half if part == 0 else ring
        start = 0 if part == 0 else half
        for i in range(start, cut):
            relay(a, "L", low[i])
            relay(a, "H", high[i])
            relay(a, "M", middle[i])

    def finish(a, q, rel):
        for g in "LMH":
            key = (a, g, q, rel)
            if key in waited:
                continue
            waited.add(key)
            cond = member(g)
            if rel == 0:
                cond = cond & (r != q)
            for done in early.get(key, []):
                cond = cond & (r != done)

            @pl.when(cond)
            def _():
                here = slot(*key)
                m = number[key]
                remote(here, here, w_send.at[m, 0], w_recv.at[m], partner, tp).wait_recv()

    for cond, copy in own_copies:
        @pl.when(cond)
        def _():
            copy.wait()
    own_sends("G", "lry")
    own_sends("U", "l")
    w_local.wait()
    w_x = remote(w_all.at[tp], w_all.at[tp], wo_ssem.at[0], wo_rsem.at[0], sp, across)
    w_x.start()
    w_d = remote(w_all.at[tp], w_all.at[tp], wo_ssem.at[1], wo_rsem.at[1], sp, core)
    w_d.start()
    w_xd = remote(w_all.at[across], w_all.at[across], wo_ssem.at[2], wo_rsem.at[2], sp, core)

    states = local_scan(qp, kp, vp, strength, decay_pre, extra, rate, out_scr)
    for h in range(heads):
        x_send[h] = states[h].astype(BF16)
    x_copy = remote(x_send, x_part, x_sem.at[0], x_sem.at[1], partner, tp)
    x_copy.start()
    own_sends("U", "y")
    x_copy.wait_recv()
    combine(states, x_part, p, p_send)

    def p_copy(k, to, slot_at):
        return remote(p_send, p_recv.at[slot_at], p_ssem.at[k], p_rsem.at[k], to, tp)

    for k in range(1, ring):
        @pl.when(r + k < ring)
        def _():
            p_copy(k, at(r + k), r).start()
    own_sends("U", "r")
    detours("G")
    relays("G", 0)
    w_x.wait_recv()
    w_xd.start()
    for k in range(1, ring):
        @pl.when(r - k >= 0)
        def _():
            p_copy(k, at(r - k), r - k).wait_recv()
    fold_states(r, p_recv, s_in, heads)
    apply_state(p, x_part, s_in, out_scr, head_gain, gp, mixed, heads)

    def token_rows(t):
        return pl.ds(pl.multiple_of(t * own_rows, own_rows), own_rows)

    mix_copies = []
    for i, to in enumerate((across, diagonal, core)):
        copy = remote(mixed.at[token_rows(to), :], mix_all.at[i], m_ssem.at[i], m_rsem.at[i], sp, to)
        copy.start()
        mix_copies.append((to, copy))
    relays("G", 1)
    total = dot1(mixed[token_rows(tp), :], w_all[tp]).astype(BF16).astype(F32)
    w_d.wait_recv()
    w_xd.wait_recv()
    for i, (to, copy) in enumerate(mix_copies):
        copy.wait_recv()
        total = total + dot1(mix_all[i], w_all[to]).astype(BF16).astype(F32)
    total = stream[...].astype(F32) + total
    residual[...] = total
    normed = (
        total * lax.rsqrt(jnp.mean(total * total, axis=-1, keepdims=True) + EPSILON) * feed_gain[...]
    ).astype(BF16)

    def block_of(z_, x_, c_):
        b = (c_ * 2 + x_) * 2 + z_
        return rows_all.at[pl.ds(pl.multiple_of(b * own_rows, own_rows), own_rows), :]

    b_own = (c * 2 + x) * 2 + zz
    rows_all[pl.ds(pl.multiple_of(b_own * own_rows, own_rows), own_rows), :] = normed
    t_copies = []

    def token(i, block, sp_to, tp_to):
        copy = remote(block, block, t_ssem.at[i], t_rsem.at[i], sp_to, tp_to)
        copy.start()
        t_copies.append(copy)

    def token_wait(i, block):
        remote(block, block, t_ssem.at[i], t_rsem.at[i], sp, across).wait_recv()

    token(0, block_of(zz, x, c), mate, tp)
    token(1, block_of(zz, x, c), sp, across)
    token(2, block_of(zz, x, c), sp, core)
    detours("U")
    relays("U", 0)
    token_wait(0, block_of(1 - zz, x, c))
    token(3, block_of(1 - zz, x, c), sp, across)
    token(4, block_of(1 - zz, x, c), sp, core)
    token_wait(1, block_of(zz, 1 - x, c))
    token(5, block_of(zz, 1 - x, c), sp, core)
    own_sends("D", "lry")
    relays("U", 1)
    token_wait(3, block_of(1 - zz, 1 - x, c))
    token(6, block_of(1 - zz, 1 - x, c), sp, core)
    token_wait(2, block_of(zz, x, 1 - c))
    token_wait(4, block_of(1 - zz, x, 1 - c))
    token_wait(5, block_of(zz, 1 - x, 1 - c))
    token_wait(6, block_of(1 - zz, 1 - x, 1 - c))
    for a in "GU":
        for rel in (0, 1):
            for q in range(ring):
                finish(a, q, rel)
    detours("D")

    has_m = member("M")
    first = jnp.where(r < half, 0, jnp.where(has_m, regions["M"][2] // 128, regions["H"][2] // 128))
    many = (regions["L"][3] - regions["L"][2]) // 128 + jnp.where(has_m, (regions["M"][3] - regions["M"][2]) // 128, 0)

    def ffn_in(i, _):
        lanes = pl.ds(pl.multiple_of((first + i) * 128, 128), 128)
        both = dot1(rows_all[...], jnp.concatenate([gate_all[:, lanes], up_all[:, lanes]], axis=1))
        hidden[:, pl.ds(pl.multiple_of(i * 128, 128), 128)] = (silu(both[:, :128]) * both[:, 128:]).astype(BF16)
        return 0

    lax.fori_loop(0, many, ffn_in, 0)
    relays("D", 0)
    relays("D", 1)

    order = [(q, 0) for q in middle] + [(q, 1) for q in middle]
    side = regions["L"][3]
    mids = regions["M"][3] - regions["M"][2]
    base = pl.multiple_of(first * 128, 128)
    f_sends = []

    def lanes_of(i):
        q, rel = order[i]
        s = q * 2 + (p if rel == 0 else 1 - p)
        return s, pl.ds(pl.multiple_of(s * dc, dc), dc)

    hop = 4 * own_rows

    def stage_a(i):
        q, rel = order[i]
        finish("D", q, rel)
        s, _ = lanes_of(i)

        @pl.when(has_m)
        def _():
            acc[i] = dot1(hidden[...], down_all[s, pl.ds(base, side + mids), :])

        @pl.when(jnp.logical_not(has_m))
        def _():
            acc[i] = dot1(hidden[:, :side], down_all[s, pl.ds(base, side), :])

        fd_send[i] = acc[i, pl.ds(pl.multiple_of((1 - c) * hop, hop), hop), :].astype(BF16)
        copy = remote(fd_send.at[i], fd_recv.at[i], fd_ssem.at[i], fd_rsem.at[i], sp, core)
        copy.start()
        f_sends.append(copy)

    def stage_b(i):
        f = remote(fd_send.at[i], fd_recv.at[i], fd_ssem.at[i], fd_rsem.at[i], sp, core)
        f.wait_recv()
        acc2[i] = acc[i, pl.ds(pl.multiple_of(c * hop, hop), hop), :] + fd_recv[i].astype(F32)
        fx_send[i] = acc2[i, pl.ds(pl.multiple_of((1 - x) * (hop // 2), hop // 2), hop // 2), :].astype(BF16)
        copy = remote(fx_send.at[i], fx_recv.at[i], fx_ssem.at[i], fx_rsem.at[i], sp, across)
        copy.start()
        f_sends.append(copy)

    def stage_c(i):
        f = remote(fx_send.at[i], fx_recv.at[i], fx_ssem.at[i], fx_rsem.at[i], sp, across)
        f.wait_recv()
        acc3[i] = acc2[i, pl.ds(pl.multiple_of(x * (hop // 2), hop // 2), hop // 2), :] + fx_recv[i].astype(F32)
        fz_send[i] = acc3[i, pl.ds(pl.multiple_of((1 - zz) * own_rows, own_rows), own_rows), :].astype(BF16)
        copy = remote(fz_send.at[i], fz_recv.at[i], fz_ssem.at[i], fz_rsem.at[i], mate, tp)
        copy.start()
        f_sends.append(copy)

    def stage_d(i):
        f = remote(fz_send.at[i], fz_recv.at[i], fz_ssem.at[i], fz_rsem.at[i], mate, tp)
        f.wait_recv()
        _, lanes = lanes_of(i)
        ffn = acc3[i, pl.ds(pl.multiple_of(zz * own_rows, own_rows), own_rows), :] + fz_recv[i].astype(F32)
        result[:, lanes] = (residual[:, lanes] + ffn).astype(BF16)

    for i in range(n + 3):
        if i < n:
            stage_a(i)
        if 0 <= i - 1 < n:
            stage_b(i - 1)
        if 0 <= i - 2 < n:
            stage_c(i - 2)
        if 0 <= i - 3 < n:
            stage_d(i - 3)

    for cond, make in sends:
        @pl.when(cond)
        def _():
            make().wait_send()
    for copy in [x_copy, w_x, w_d, w_xd] + [m for _, m in mix_copies] + t_copies + f_sends:
        copy.wait_send()
    for k in range(1, ring):
        @pl.when(r + k < ring)
        def _():
            p_copy(k, at(r + k), r).wait_send()


def paired_body(n, tps, stream, qp, kp, vp, gp, strength, decay_pre, extra, rate, head_gain, w_out,
                feed_gain, gate_m, up_m, down_m):
    heads, tokens = strength.shape
    own, width = stream.shape
    kr, units = gate_m.shape
    dc = down_m.shape[1]
    ring = n // 2
    side = (units // 128 - 1) // 2 * 128
    most = units - side
    group = 2 * tps * own
    dma = pltpu.SemaphoreType.DMA
    vmem = pl.BlockSpec(memory_space=pltpu.VMEM)
    hbm = pl.BlockSpec(memory_space=pl.ANY)
    keys = 3 * 3 * ring * 2
    return pl.pallas_call(
        functools.partial(paired_kernel, n, tps),
        out_shape=jax.ShapeDtypeStruct((own, width), BF16),
        in_specs=[vmem] * 11 + [hbm] * 4,
        out_specs=vmem,
        scratch_shapes=[
            pltpu.VMEM((kr * n, units), BF16),
            pltpu.VMEM((kr * n, units), BF16),
            pltpu.VMEM((n,) + down_m.shape, BF16),
            pltpu.VMEM((tps,) + w_out.shape, BF16),
            pltpu.VMEM((heads, tokens, 2 * HEAD), F32),
            pltpu.VMEM((heads, HEAD, 2 * HEAD), BF16),
            pltpu.VMEM((heads, HEAD, 2 * HEAD), BF16),
            pltpu.VMEM((heads, HEAD, 2 * HEAD), BF16),
            pltpu.VMEM((ring, heads, HEAD, 2 * HEAD), BF16),
            pltpu.VMEM((heads, HEAD, HEAD), F32),
            pltpu.VMEM((tokens, heads * HEAD), BF16),
            pltpu.VMEM((tps - 1, own, heads * HEAD), BF16),
            pltpu.VMEM((own, width), F32),
            pltpu.VMEM((group, width), BF16),
            pltpu.VMEM((group, most), BF16),
            pltpu.VMEM((n, group, dc), F32),
            pltpu.VMEM((n, group // 2, dc), F32),
            pltpu.VMEM((n, group // 4, dc), F32),
            pltpu.VMEM((n, group // 2, dc), BF16),
            pltpu.VMEM((n, group // 2, dc), BF16),
            pltpu.VMEM((n, group // 4, dc), BF16),
            pltpu.VMEM((n, group // 4, dc), BF16),
            pltpu.VMEM((n, group // 8, dc), BF16),
            pltpu.VMEM((n, group // 8, dc), BF16),
            dma((keys, 4)), dma((keys,)), dma((10,)), dma((2,)), dma((ring,)), dma((ring,)),
            dma((3,)), dma((3,)), dma((3,)), dma((3,)), dma((7,)), dma((7,)),
            dma((n,)), dma((n,)), dma((n,)), dma((n,)), dma((n,)), dma((n,)),
        ],
        compiler_params=pltpu.CompilerParams(
            collective_id=0, has_side_effects=True, vmem_limit_bytes=60 * 1024 * 1024),
    )(stream, qp, kp, vp, gp, strength, decay_pre, extra, rate[:, None], head_gain[None, :],
      feed_gain[None, :], w_out, gate_m, up_m, down_m)


def body(n, tps, *args):
    ring = n // 2
    short = ring % 4 == 0 and ring <= UNROLLED and tps == 4
    return (paired_body if short else chain_body)(n, tps, *args)


def solution(mesh):
    placed = (
        P(("sp", "tp"), None),
        P("sp", "tp"),
        P("sp", "tp"),
        P("sp", "tp"),
        P("sp", "tp"),
        P("tp", "sp"),
        P("tp", "sp"),
        P("tp", "sp"),
        P("tp"),
        P(),
        P("tp", None),
        P(),
        P("sp", "tp"),
        P("sp", "tp"),
        P("tp", "sp"),
    )
    return jax.shard_map(
        functools.partial(body, mesh.shape["sp"], mesh.shape["tp"]),
        mesh=mesh, in_specs=placed, out_specs=P(("sp", "tp"), None), check_vma=False,
    )
```

```python
import functools

import jax
import jax.numpy as jnp
from jax import lax
from jax.experimental import pallas as pl
from jax.experimental.pallas import tpu as pltpu
from jax.sharding import PartitionSpec as P

HEAD = 128
CHUNK = 128
UNROLLED = 4
EPSILON = 1e-06
F32 = jnp.float32
BF16 = jnp.bfloat16
HIGHEST = lax.Precision.HIGHEST
NN = (((1,), (0,)), ((), ()))
NT = (((1,), (1,)), ((), ()))
TN = (((0,), (0,)), ((), ()))


def dot1(a, b, dims=NN):
    return lax.dot_general(a, b, dims, preferred_element_type=F32)


def halves(x):
    high = x.astype(BF16)
    return high, (x - high.astype(F32)).astype(BF16)


def dot3(a, b, dims=NN):
    ah, al = halves(a)
    bh, bl = halves(b)
    return dot1(ah, bh, dims) + (dot1(ah, bl, dims) + dot1(al, bh, dims))


def silu(x):
    return x * jax.nn.sigmoid(x)


def local_scan(qp, kp, vp, strength, decay_pre, extra, rate, out_scr):
    heads, tokens = strength.shape
    chunks = tokens // CHUNK
    row_i = lax.broadcasted_iota(jnp.int32, (CHUNK, CHUNK), 0)
    col_i = lax.broadcasted_iota(jnp.int32, (CHUNK, CHUNK), 1)
    causal = row_i >= col_i
    strict = row_i > col_i
    eye = jnp.where(row_i == col_i, 1.0, 0.0).astype(F32)
    lower = jnp.where(causal, 1.0, 0.0).astype(F32)
    beta = jax.nn.sigmoid(strength[...].astype(F32))
    pre = decay_pre[...].astype(F32)
    soft = jnp.maximum(pre, 0.0) + jnp.log1p(jnp.exp(-jnp.abs(pre)))
    log_decay = -rate[...] * soft + extra[...]

    pairs = [(h, c) for c in range(chunks) for h in range(heads)]
    data = {}
    for c in range(chunks):
        span = slice(c * CHUNK, (c + 1) * CHUNK)
        ld = log_decay[:, span]
        c_row = lax.dot_general(ld, lower, NT, precision=HIGHEST, preferred_element_type=F32)
        c_col = lax.dot_general(lower, ld, NT, precision=HIGHEST, preferred_element_type=F32)
        b_col = lax.dot_general(eye, beta[:, span], NT, precision=HIGHEST, preferred_element_type=F32)
        for h in range(heads):
            lanes = slice(h * HEAD, (h + 1) * HEAD)
            q = qp[span, lanes].astype(F32)
            k = kp[span, lanes].astype(F32)
            v = vp[span, lanes].astype(F32)
            q = q * (lax.rsqrt(jnp.sum(q * q, axis=-1, keepdims=True) + EPSILON) * HEAD ** (-0.5))
            k = k * lax.rsqrt(jnp.sum(k * k, axis=-1, keepdims=True) + EPSILON)
            cc = c_col[:, h:h + 1]
            bb = b_col[:, h:h + 1]
            cr = c_row[h:h + 1, :]
            last = cr[:, CHUNK - 1:]
            damp = jnp.where(causal, jnp.exp(jnp.where(causal, cc - cr, 0.0)), 0.0)
            grown = jnp.exp(cc)
            kb = k * bb
            kk = dot3(kb, k, NT) * jnp.where(strict, damp, 0.0)
            inner = dot3(q, k, NT) * damp
            data[h, c] = dict(
                low=kk, inner=inner, v=v * bb, kw=kb * grown, qd=q * grown,
                kd=k * jnp.exp(last - cc), decay=jnp.exp(last),
            )
    inverse = {}
    b = 1
    shift = 0
    while b < CHUNK:
        mask = ((row_i >> (shift + 1)) == (col_i >> (shift + 1))) & (
            ((row_i >> shift) & 1) == 1) & (((col_i >> shift) & 1) == 0)
        for key in pairs:
            piece = jnp.where(mask, data[key]["low"], 0.0)
            if b == 1:
                inverse[key] = eye - piece
            else:
                x = inverse[key]
                inverse[key] = x - dot3(x, dot3(piece, x))
        b *= 2
        shift += 1
    states = [jnp.concatenate([jnp.zeros((HEAD, HEAD), F32), eye], axis=1) for _ in range(heads)]
    for c in range(chunks):
        for h in range(heads):
            e = data[h, c]
            u = dot3(inverse[h, c], e["v"])
            w = dot3(inverse[h, c], e["kw"])
            x = states[h]
            new = jnp.concatenate([u, jnp.zeros_like(u)], axis=1) - dot3(w, x)
            out_scr[h, c * CHUNK:(c + 1) * CHUNK, :] = dot3(e["qd"], x) + dot3(e["inner"], new)
            states[h] = e["decay"] * x + dot3(e["kd"], new, TN)
    return states


def combine(states, x_part, p, p_send):
    heads = len(states)
    for h in range(heads):
        mine = states[h]
        theirs = x_part[h].astype(F32)
        before = jnp.where(p == 0, mine, theirs)
        after = jnp.where(p == 0, theirs, mine)
        after_s = jnp.concatenate([after[:, :HEAD], jnp.zeros((HEAD, HEAD), F32)], axis=1)
        p_send[h] = (dot3(after[:, HEAD:], before) + after_s).astype(BF16)


def fold_states(r, p_recv, s_in, heads):
    s_in[...] = jnp.zeros_like(s_in)

    def fold(i, _):
        for h in range(heads):
            got = p_recv[i, h].astype(F32)
            s_in[h] = dot3(got[:, HEAD:], s_in[h]) + got[:, :HEAD]
        return 0

    lax.fori_loop(0, r, fold, 0)


def fold_from_first(r, p_recv, s_in, heads):
    s_in[...] = jnp.zeros_like(s_in)

    @pl.when(r > 0)
    def _():
        for h in range(heads):
            s_in[h] = p_recv[0, h, :, :HEAD].astype(F32)

    def fold(i, _):
        for h in range(heads):
            got = p_recv[i, h].astype(F32)
            s_in[h] = dot3(got[:, HEAD:], s_in[h]) + got[:, :HEAD]
        return 0

    lax.fori_loop(1, r, fold, 0)


def apply_state(p, x_part, s_in, out_scr, head_gain, gp, mixed, heads):
    for h in range(heads):
        lanes = slice(h * HEAD, (h + 1) * HEAD)
        got = x_part[h].astype(F32)
        s = s_in[h]
        s = jnp.where(p == 0, s, dot3(got[:, HEAD:], s) + got[:, :HEAD])
        att = out_scr[h, :, :HEAD] + dot3(out_scr[h, :, HEAD:], s)
        att = att * lax.rsqrt(jnp.mean(att * att, axis=-1, keepdims=True) + EPSILON) * head_gain[...]
        mixed[:, lanes] = (att * silu(gp[:, lanes].astype(F32))).astype(BF16)


def messages(ring):
    own_z = [(a, 0, 0, way) for a in "GU" for way in "RL"]
    own_y = [(a, 0, 0, "Y") for a in "GU"]
    first = own_z + own_y
    down_y = [("D", 0, 0, "Y")]

    def relay(a, j, skip_y=False):
        out = []
        if j < ring - 1:
            out += [(a, -j, 0, "R"), (a, j, 0, "L")]
        if not skip_y:
            out += [(a, -j, 0, "Y"), (a, j, 0, "Y")]
        return out

    early, middle, later, last = [], [], [], []
    if ring > 1:
        early = relay("G", 1)
        middle = relay("U", 1)
        for j in range(2, ring):
            later += relay("G", j) + relay("U", j)
            if j == 2:
                later += [("D", 0, 0, "R"), ("D", 0, 0, "L")]
        if ring == 2:
            later += [("D", 0, 0, "R"), ("D", 0, 0, "L")]
        later += [("D", 0, 1, "R"), ("D", 0, 1, "L")]
        later += relay("D", 1, skip_y=True)
        for j in range(2, ring):
            last += relay("D", j)
    else:
        first = own_y
    return first, down_y, early, middle, later, last


def chain_kernel(
    n, tps, groups,
    stream, qp, kp, vp, gp, strength, decay_pre, extra, rate, head_gain, w_out, feed_gain,
    gate_in, up_in, down_in,
    result,
    gate_all, up_all, down_all, out_scr, x_send, x_part, p_send, p_recv, s_in, mixed,
    d_send, d_recv, residual, rows_all, hidden, f_part, f_recv,
    w_send, w_recv, own_sem, x_sem, p_ssem, p_rsem, d_ssem, d_rsem, e_ssem, e_rsem, f_ssem, f_rsem,
):
    ring = n // 2
    sp = lax.axis_index("sp")
    tp = lax.axis_index("tp")
    r = sp // 2
    p = lax.rem(sp, 2)
    heads = strength.shape[0]
    tokens = strength.shape[1]
    chunks = tokens // CHUNK
    own_rows = stream.shape[0]
    kr = gate_in.shape[0]
    MESH = pl.DeviceIdType.MESH

    def sp_of(dr, rel):
        q = p if rel == 0 else 1 - p
        return lax.rem(r + dr + ring, ring) * 2 + q

    partner = sp_of(0, 1)
    where = {"R": sp_of(1, 0), "L": sp_of(-1, 0), "Y": partner}

    def tp_peer(o):
        return lax.rem(tp + o, tps)

    barrier = pltpu.get_barrier_semaphore()
    for dr in range(1, ring):
        pl.semaphore_signal(barrier, 1, device_id=(sp_of(dr, 0), tp), device_id_type=MESH)
    pl.semaphore_signal(barrier, 1, device_id=(partner, tp), device_id_type=MESH)
    for o in range(1, tps):
        pl.semaphore_signal(barrier, 1, device_id=(sp, tp_peer(o)), device_id_type=MESH)
    pl.semaphore_wait(barrier, ring + tps - 1)

    flat = [m for g in groups for m in g]
    number = {m: i for i, m in enumerate(flat)}
    arrival = {}
    for (a, dr, rel, way) in flat:
        to = {"R": (dr - 1, rel), "L": (dr + 1, rel), "Y": (dr, 1 - rel)}[way]
        key = (a, to[0], to[1])
        assert key not in arrival
        arrival[key] = number[(a, dr, rel, way)]
    waited = set()
    copies = []

    def exists(dr):
        return (r + dr >= 0) & (r + dr < ring)

    def slot(a, dr, rel):
        s = sp_of(dr, rel)
        if a == "D":
            return down_all.at[s]
        whole = gate_all if a == "G" else up_all
        return whole.at[pl.ds(pl.multiple_of(s * kr, kr), kr), :]

    inputs = {"G": gate_in, "U": up_in, "D": down_in}

    def need(a, dr, rel):
        key = (a, dr, rel)
        if (dr == 0 and rel == 0) or key in waited:
            return
        waited.add(key)
        m = arrival[key]

        @pl.when(exists(dr))
        def _():
            here = slot(*key)
            pltpu.make_async_remote_copy(
                here, here, w_send.at[m], w_recv.at[m], device_id=(partner, tp), device_id_type=MESH
            ).wait_recv()

    def outgoing(message):
        a, dr, rel, way = message
        m = number[message]
        return pltpu.make_async_remote_copy(
            inputs[a] if dr == 0 and rel == 0 else slot(a, dr, rel),
            slot(a, dr, rel),
            w_send.at[m], w_recv.at[m],
            device_id=(where[way], tp), device_id_type=MESH,
        )

    def goes(message):
        ahead = {"R": r + 1 < ring, "L": r >= 1, "Y": r >= 0}[message[3]]
        return exists(message[1]) & ahead

    def pump(group):
        for message in group:
            need(*message[:3])

            @pl.when(goes(message))
            def _():
                outgoing(message).start()

            copies.append(message)

    def need_all(a):
        for dr in sorted(range(1 - ring, ring), key=abs):
            for rel in (0, 1):
                need(a, dr, rel)

    first, down_y, early, middle, later, last_group = groups
    pump(first)
    locals_ = []
    for i, a in enumerate("GUD"):
        local = pltpu.make_async_copy(inputs[a], slot(a, 0, 0), own_sem.at[i])
        local.start()
        locals_.append(local)

    states = local_scan(qp, kp, vp, strength, decay_pre, extra, rate, out_scr)
    for h in range(heads):
        x_send[h] = states[h].astype(BF16)
    x_copy = pltpu.make_async_remote_copy(
        x_send, x_part, x_sem.at[0], x_sem.at[1], device_id=(partner, tp), device_id_type=MESH)
    x_copy.start()
    pump(down_y)
    x_copy.wait_recv()
    combine(states, x_part, p, p_send)

    def p_copy(k, to, at):
        return pltpu.make_async_remote_copy(
            p_send, p_recv.at[at], p_ssem.at[k], p_rsem.at[k],
            device_id=(to, tp), device_id_type=MESH)

    for k in range(1, ring):
        @pl.when(r + k < ring)
        def _():
            p_copy(k, sp_of(k, 0), r).start()
    pump(early)
    for k in range(1, ring):
        @pl.when(r - k >= 0)
        def _():
            p_copy(k, sp_of(-k, 0), r - k).wait_recv()
    fold_states(r, p_recv, s_in, heads)
    apply_state(p, x_part, s_in, out_scr, head_gain, gp, mixed, heads)

    def rows_of(t):
        return pl.ds(pl.multiple_of(t * own_rows, own_rows), own_rows)

    order = [o for o in (2, 3, 1) if o < tps] + list(range(4, tps))
    d_copies = []
    for o in order:
        to = tp_peer(o)
        d_send[o - 1] = dot1(mixed[rows_of(to), :], w_out[...]).astype(BF16)
        copy = pltpu.make_async_remote_copy(
            d_send.at[o - 1], d_recv.at[o - 1], d_ssem.at[o - 1], d_rsem.at[o - 1],
            device_id=(sp, to), device_id_type=MESH)
        copy.start()
        d_copies.append(copy)
    pump(middle)
    total = dot1(mixed[rows_of(tp), :], w_out[...]).astype(BF16).astype(F32)
    for copy in d_copies:
        copy.wait_recv()
    for o in range(1, tps):
        total = total + d_recv[o - 1].astype(F32)
    total = stream[...].astype(F32) + total
    residual[...] = total
    rows_all[rows_of(tp), :] = (
        total * lax.rsqrt(jnp.mean(total * total, axis=-1, keepdims=True) + EPSILON) * feed_gain[...]
    ).astype(BF16)
    e_copies = []
    for o in order:
        copy = pltpu.make_async_remote_copy(
            rows_all.at[rows_of(tp), :], rows_all.at[rows_of(tp), :], e_ssem.at[o - 1], e_rsem.at[o - 1],
            device_id=(sp, tp_peer(o)), device_id_type=MESH)
        copy.start()
        e_copies.append(copy)
    for o in order:
        there = rows_all.at[rows_of(lax.rem(tp - o + tps, tps)), :]
        pltpu.make_async_remote_copy(
            there, there, e_ssem.at[o - 1], e_rsem.at[o - 1],
            device_id=(sp, tp_peer(o)), device_id_type=MESH).wait_recv()
    pump(later)
    need_all("G")
    need_all("U")
    for local in locals_:
        local.wait()

    tile = 128

    def ffn_in(i, _):
        lanes = pl.ds(pl.multiple_of(i * tile, tile), tile)
        both = dot1(rows_all[...], jnp.concatenate([gate_all[:, lanes], up_all[:, lanes]], axis=1))
        hidden[:, lanes] = (silu(both[:, :tile]) * both[:, tile:]).astype(BF16)
        return 0

    lax.fori_loop(0, gate_all.shape[1] // tile, ffn_in, 0)
    pump(last_group)
    need_all("D")
    dc = down_all.shape[2]
    pack = max(1, 128 // dc)
    wide = pack * dc

    def ffn_out(i, _):
        lanes = pl.ds(pl.multiple_of(i * wide, wide), wide)
        if pack == 1:
            weights = down_all[i]
        else:
            weights = jnp.concatenate([down_all[i * pack + j] for j in range(pack)], axis=1)
        f_part[:, lanes] = dot1(hidden[...], weights).astype(BF16)
        return 0

    lax.fori_loop(0, n // pack, ffn_out, 0)
    f_copies = []
    for o in order:
        copy = pltpu.make_async_remote_copy(
            f_part.at[rows_of(tp_peer(o)), :], f_recv.at[o - 1], f_ssem.at[o - 1], f_rsem.at[o - 1],
            device_id=(sp, tp_peer(o)), device_id_type=MESH)
        copy.start()
        f_copies.append(copy)
    ffn = f_part[rows_of(tp), :].astype(F32)
    for copy in f_copies:
        copy.wait_recv()
    for o in range(1, tps):
        ffn = ffn + f_recv[o - 1].astype(F32)
    result[...] = (residual[...] + ffn).astype(BF16)

    for message in copies:
        @pl.when(goes(message))
        def _():
            outgoing(message).wait_send()
    for copy in [x_copy] + d_copies + e_copies + f_copies:
        copy.wait_send()
    for k in range(1, ring):
        @pl.when(r + k < ring)
        def _():
            p_copy(k, sp_of(k, 0), r).wait_send()


def chain_body(n, tps, stream, qp, kp, vp, gp, strength, decay_pre, extra, rate, head_gain, w_out,
         feed_gain, gate_m, up_m, down_m):
    heads, tokens = strength.shape
    own, width = stream.shape
    kr, units = gate_m.shape
    ring = n // 2
    groups = messages(ring)
    count = sum(len(g) for g in groups)
    dma = pltpu.SemaphoreType.DMA
    vmem = pl.BlockSpec(memory_space=pltpu.VMEM)
    hbm = pl.BlockSpec(memory_space=pl.ANY)
    peers = max(1, tps - 1)
    return pl.pallas_call(
        functools.partial(chain_kernel, n, tps, groups),
        out_shape=jax.ShapeDtypeStruct((own, width), BF16),
        in_specs=[vmem] * 12 + [hbm] * 3,
        out_specs=vmem,
        scratch_shapes=[
            pltpu.VMEM((kr * n, units), BF16),
            pltpu.VMEM((kr * n, units), BF16),
            pltpu.VMEM((n,) + down_m.shape, BF16),
            pltpu.VMEM((heads, tokens, 2 * HEAD), F32),
            pltpu.VMEM((heads, HEAD, 2 * HEAD), BF16),
            pltpu.VMEM((heads, HEAD, 2 * HEAD), BF16),
            pltpu.VMEM((heads, HEAD, 2 * HEAD), BF16),
            pltpu.VMEM((ring, heads, HEAD, 2 * HEAD), BF16),
            pltpu.VMEM((heads, HEAD, HEAD), F32),
            pltpu.VMEM((tokens, heads * HEAD), BF16),
            pltpu.VMEM((peers, own, width), BF16),
            pltpu.VMEM((peers, own, width), BF16),
            pltpu.VMEM((own, width), F32),
            pltpu.VMEM((tokens, width), BF16),
            pltpu.VMEM((tokens, units), BF16),
            pltpu.VMEM((tokens, width), BF16),
            pltpu.VMEM((peers, own, width), BF16),
            dma((count,)), dma((count,)), dma((3,)), dma((2,)), dma((ring,)), dma((ring,)),
            dma((peers,)), dma((peers,)), dma((peers,)), dma((peers,)), dma((peers,)), dma((peers,)),
        ],
        compiler_params=pltpu.CompilerParams(
            collective_id=0, has_side_effects=True, vmem_limit_bytes=60 * 1024 * 1024),
    )(stream, qp, kp, vp, gp, strength, decay_pre, extra, rate[:, None], head_gain[None, :], w_out,
      feed_gain[None, :], gate_m, up_m, down_m)


def regions_of(ring, units):
    tiles = units // 128
    side = (tiles - 1) // 2 * 128
    half, quarter = ring // 2, ring // 4
    return {
        "L": (0, half, 0, side),
        "M": (quarter, half + quarter, side, units - side),
        "H": (half, ring, units - side, units),
    }


def paired_kernel(
    n, tps,
    stream, qp, kp, vp, gp, strength, decay_pre, extra, rate, head_gain, feed_gain,
    w_out, gate_in, up_in, down_in,
    result,
    gate_all, up_all, down_all, w_all, out_scr, x_send, x_part, p_send, p_recv, s_in, mixed, mix_all,
    residual, rows_all, hidden, acc, acc2, acc3, fd_send, fd_recv, fx_send, fx_recv, fz_send, fz_recv,
    w_send, w_recv, own_sem, x_sem, p_ssem, p_rsem, wo_ssem, wo_rsem, m_ssem, m_rsem, t_ssem, t_rsem,
    fd_ssem, fd_rsem, fx_ssem, fx_rsem, fz_ssem, fz_rsem,
):
    ring = n // 2
    half = ring // 2
    sp = lax.axis_index("sp")
    tp = lax.axis_index("tp")
    r = sp // 2
    p = lax.rem(sp, 2)
    x = tp // 2
    c = lax.rem(tp, 2)
    zz = jnp.where(r >= half, 1, 0)
    heads = strength.shape[0]
    own_rows = stream.shape[0]
    kr, units = gate_in.shape
    width = stream.shape[1]
    dc = down_in.shape[1]
    MESH = pl.DeviceIdType.MESH
    regions = regions_of(ring, units)
    partner = r * 2 + 1 - p
    mate = lax.rem(r + half, ring) * 2 + p
    core = x * 2 + 1 - c
    across = (1 - x) * 2 + c
    diagonal = (1 - x) * 2 + 1 - c

    def at(q):
        return q * 2 + p

    def remote(src, dst, ssem, rsem, sp_to, tp_to):
        return pltpu.make_async_remote_copy(src, dst, ssem, rsem, device_id=(sp_to, tp_to), device_id_type=MESH)

    inputs = {"G": gate_in, "U": up_in, "D": down_in}
    def spans(g, k):
        return (k >= regions[g][0]) & (k < regions[g][1])

    taken = {"send": [], "recv": []}

    def color(kind, users):
        for i, held in enumerate(taken[kind]):
            if not held & users:
                held |= users
                return i
        taken[kind].append(set(users))
        return len(taken[kind]) - 1

    number = {}
    for a in "GUD":
        for g in "LMH":
            for q in range(ring):
                for rel in (0, 1):
                    users = {k for k in range(ring) if spans(g, k) and (rel == 1 or k != q)}
                    number[a, g, q, rel] = color("recv", users)

    def slot(a, g, q, rel):
        s = q * 2 + (p if rel == 0 else 1 - p)
        c0, c1 = regions[g][2:]
        if a == "D":
            return down_all.at[s, c0:c1, :]
        whole = gate_all if a == "G" else up_all
        return whole.at[pl.ds(pl.multiple_of(s * kr, kr), kr), c0:c1]

    def own(a, g):
        c0, c1 = regions[g][2:]
        return inputs[a].at[c0:c1, :] if a == "D" else inputs[a].at[:, c0:c1]

    def member(g):
        return spans(g, r)

    own_copies = []
    for i, a in enumerate("GUD"):
        for j, g in enumerate("LMH"):
            for q in range(*regions[g][:2]):
                copy = pltpu.make_async_copy(own(a, g), slot(a, g, q, 0), own_sem.at[3 * i + j])
                own_copies.append((r == q, copy))

                @pl.when(r == q)
                def _():
                    copy.start()

    w_local = pltpu.make_async_copy(w_out, w_all.at[tp], own_sem.at[9])
    w_local.start()

    barrier = pltpu.get_barrier_semaphore()
    for k in range(1, ring):
        pl.semaphore_signal(barrier, 1, device_id=(at(lax.rem(r + k, ring)), tp), device_id_type=MESH)
    pl.semaphore_signal(barrier, 1, device_id=(partner, tp), device_id_type=MESH)
    for k in range(1, tps):
        pl.semaphore_signal(barrier, 1, device_id=(sp, lax.rem(tp + k, tps)), device_id_type=MESH)
    pl.semaphore_wait(barrier, ring + tps - 1)

    def detour(a, g, q, to):
        lo, hi = regions[g][:2]
        if g == "M" or hi - lo < 2:
            return False
        inner, outer = (hi - 1, hi - 2) if g == "L" else (lo, lo + 1)
        return a != "G" and (q, to) == (outer, inner)

    sends = []
    waited = set()

    def send(cond, src, key, way, sp_to):
        users = {k for k in range(ring) if cond(k)}
        if not users:
            return
        m = color("send", users)
        landing = key[:3] + (1,) if way == "y" else key

        def make():
            return remote(src, slot(*key), w_send.at[m], w_recv.at[number[landing]], sp_to, tp)

        @pl.when(cond(r))
        def _():
            make().start()

        sends.append((cond(r), make))

    def forwards_y(a, g, q, k):
        return spans(g, k) and not detour(a, g, q, k)

    def own_sends(a, ways, only=None):
        for g in "LMH":
            lo, hi = regions[g][:2]
            for q in range(ring):
                if only is not None and (q >= half) != only:
                    continue
                key = (a, g, q, 0)
                mine = functools.partial(lambda q, k: k == q, q)
                inside = lo <= q < hi
                here = slot(*key) if inside else own(a, g)
                if inside and "y" in ways:
                    send(mine, here, key, "y", partner)
                if g == "M":
                    targets = [to for to in range(lo, hi) if to != q]
                elif inside:
                    targets = [to for to in (q - 1, q + 1) if lo <= to < hi]
                else:
                    targets = [lo if q < lo else hi - 1]
                for to in targets:
                    way = "l" if to < q else "r"
                    if (way if abs(q - to) == 1 else way.upper()) in ways:
                        send(mine, here, key, way, at(to))

    def arrived(key, cond):
        here = slot(*key)

        @pl.when(cond)
        def _():
            remote(here, here, w_send.at[0], w_recv.at[number[key]], partner, tp).wait_recv()

    def role_of(g, role, k):
        lo, hi = regions[g][:2]
        inner = hi - 1 if g == "L" else lo
        return True if role is None else (k == inner) if role == "in" else (k != inner)

    def relay(a, g, q, role):
        key = (a, g, q, 0)
        lo, hi = regions[g][:2]
        assert (key, role) not in waited
        waited.add((key, role))

        def holds(k):
            return spans(g, k) & (k != q) & role_of(g, role, k)

        if any(holds(k) for k in range(ring)):
            arrived(key, holds(r))
        here = slot(*key)
        if g != "M":
            send(lambda k: holds(k) & (k > lo) & (k < q), here, key, "l", at(r - 1))
            send(lambda k: holds(k) & (k > q) & (k < hi - 1), here, key, "r", at(r + 1))
        for k in range(lo, hi):
            if holds(k) and forwards_y(a, g, q, k):
                send(functools.partial(lambda k, kk: kk == k, k), here, key, "y", partner)

    def detours(a):
        for g in "LH":
            for q in range(*regions[g][:2]):
                for to in (q - 1, q + 1):
                    if detour(a, g, q, to):
                        key = (a, g, q, 1)
                        arrived(key, r == q)
                        early.setdefault(key, []).append(q)
                        send(functools.partial(lambda q, k: k == q, q), slot(*key), key, "z", at(to))

    early = {}
    low = list(range(half - 1, -1, -1)) + list(range(half, ring))

    def relays(a, role, g, *steps):
        for i in steps:
            relay(a, g, low[i] if g == "L" else ring - 1 - low[i], role)

    def middles(a):
        for q in range(ring):
            relay(a, "M", q, None)

    def finish(a, q, rel):
        for g in "LMH":
            key = (a, g, q, rel)
            if rel == 1:
                cond = member(g)
                for done in early.get(key, []):
                    cond = cond & (r != done)
                arrived(key, cond)
                continue
            for role in (None,) if g == "M" else ("in", "out"):
                if (key, role) not in waited:
                    waited.add((key, role))
                    mine = member(g) & (r != q)
                    arrived(key, mine & role_of(g, role, r))

    for cond, copy in own_copies:
        @pl.when(cond)
        def _():
            copy.wait()
    own_sends("G", "LR")
    own_sends("G", "lry")
    w_local.wait()
    w_x = remote(w_all.at[tp], w_all.at[tp], wo_ssem.at[0], wo_rsem.at[0], sp, across)
    w_x.start()
    w_d = remote(w_all.at[tp], w_all.at[tp], wo_ssem.at[1], wo_rsem.at[1], sp, core)
    w_d.start()
    w_xd = remote(w_all.at[across], w_all.at[across], wo_ssem.at[2], wo_rsem.at[2], sp, core)

    states = local_scan(qp, kp, vp, strength, decay_pre, extra, rate, out_scr)
    for h in range(heads):
        x_send[h] = states[h].astype(BF16)
    x_copy = remote(x_send, x_part, x_sem.at[0], x_sem.at[1], partner, tp)
    x_copy.start()
    own_sends("U", "lL")
    own_sends("U", "r", True)
    x_copy.wait_recv()
    own_sends("U", "y")
    combine(states, x_part, p, p_send)

    def p_copy(k, to, slot_at):
        return remote(p_send, p_recv.at[slot_at], p_ssem.at[k], p_rsem.at[k], to, tp)

    def p_first(k, to):
        return remote(p_send.at[:, :, :HEAD], p_recv.at[0, :, :, :HEAD], p_ssem.at[k], p_rsem.at[k], to, tp)

    for k in range(ring - 1, 0, -1):
        @pl.when(r == 0)
        def _():
            p_first(k, at(k)).start()

        @pl.when((r > 0) & (r + k < ring))
        def _():
            p_copy(k, at(r + k), r).start()
    relays("G", "out", "L", 0)
    relays("G", "out", "H", 0)
    relays("G", "in", "L", 1, 2, 3)
    relays("G", "in", "H", 1)
    own_sends("D", "y")
    w_x.wait_recv()
    w_xd.start()
    for k in range(1, ring):
        @pl.when(r == k)
        def _():
            p_first(k, at(0)).wait_recv()

        @pl.when(r - k > 0)
        def _():
            p_copy(k, at(r - k), r - k).wait_recv()
    relays("G", "in", "H", 2)
    fold_from_first(r, p_recv, s_in, heads)
    apply_state(p, x_part, s_in, out_scr, head_gain, gp, mixed, heads)

    def token_rows(t):
        return pl.ds(pl.multiple_of(t * own_rows, own_rows), own_rows)

    mix_copies = []
    for i, to in enumerate((across, diagonal, core)):
        copy = remote(mixed.at[token_rows(to), :], mix_all.at[i], m_ssem.at[i], m_rsem.at[i], sp, to)
        copy.start()
        mix_copies.append((to, copy))
    for k in range(1, ring):
        @pl.when(r == 0)
        def _():
            p_first(k, at(k)).wait_send()

        @pl.when((r > 0) & (r + k < ring))
        def _():
            p_copy(k, at(r + k), r).wait_send()
    own_sends("U", "R")
    own_sends("U", "r", False)
    relays("G", "out", "L", 2)
    relays("G", "out", "H", 2)
    relays("U", "out", "L", 0)
    total = dot1(mixed[token_rows(tp), :], w_all[tp]).astype(BF16).astype(F32)
    w_d.wait_recv()
    w_xd.wait_recv()
    for i, (to, copy) in enumerate(mix_copies):
        copy.wait_recv()
        total = total + dot1(mix_all[i], w_all[to]).astype(BF16).astype(F32)
    total = stream[...].astype(F32) + total
    residual[...] = total
    normed = (
        total * lax.rsqrt(jnp.mean(total * total, axis=-1, keepdims=True) + EPSILON) * feed_gain[...]
    ).astype(BF16)

    def block_of(z_, x_, c_):
        b = (c_ * 2 + x_) * 2 + z_
        return rows_all.at[pl.ds(pl.multiple_of(b * own_rows, own_rows), own_rows), :]

    b_own = (c * 2 + x) * 2 + zz
    rows_all[pl.ds(pl.multiple_of(b_own * own_rows, own_rows), own_rows), :] = normed
    t_copies = []

    def token(i, block, sp_to, tp_to):
        copy = remote(block, block, t_ssem.at[i], t_rsem.at[i], sp_to, tp_to)
        copy.start()
        t_copies.append(copy)

    def token_wait(i, block):
        remote(block, block, t_ssem.at[i], t_rsem.at[i], sp, across).wait_recv()

    token(0, block_of(zz, x, c), mate, tp)
    token(1, block_of(zz, x, c), sp, across)
    token(2, block_of(zz, x, c), sp, core)
    relays("G", "out", "L", 3)
    relays("G", "in", "H", 3)
    relays("U", "in", "L", 1, 2)
    relays("U", "in", "H", 1)
    relays("U", "out", "H", 0)
    middles("G")
    detours("U")
    token_wait(1, block_of(zz, 1 - x, c))
    token(5, block_of(zz, 1 - x, c), sp, core)
    own_sends("D", "LR")
    own_sends("D", "lr")
    relays("G", "out", "H", 3)
    relays("U", "in", "H", 2)
    relays("U", "in", "L", 3)
    relays("U", "out", "L", 2)
    token_wait(0, block_of(1 - zz, x, c))
    token(3, block_of(1 - zz, x, c), sp, across)
    token(4, block_of(1 - zz, x, c), sp, core)
    relays("U", "in", "H", 3)
    relays("U", "out", "L", 3)
    relays("U", "out", "H", 2)
    middles("U")
    token_wait(3, block_of(1 - zz, 1 - x, c))
    token(6, block_of(1 - zz, 1 - x, c), sp, core)
    relays("U", "out", "H", 3)
    relays("D", "out", "L", 0)
    relays("D", "out", "H", 0)
    relays("D", "in", "L", 1, 2)
    relays("D", "in", "H", 1)
    detours("D")
    token_wait(2, block_of(zz, x, 1 - c))
    token_wait(4, block_of(1 - zz, x, 1 - c))
    token_wait(5, block_of(zz, 1 - x, 1 - c))
    token_wait(6, block_of(1 - zz, 1 - x, 1 - c))
    for a in "GU":
        for rel in (0, 1):
            for q in range(ring):
                finish(a, q, rel)

    has_m = member("M")
    first = jnp.where(r < half, 0, jnp.where(has_m, regions["M"][2] // 128, regions["H"][2] // 128))
    many = (regions["L"][3] - regions["L"][2]) // 128 + jnp.where(has_m, (regions["M"][3] - regions["M"][2]) // 128, 0)

    def ffn_in(i, _):
        lanes = pl.ds(pl.multiple_of((first + i) * 128, 128), 128)
        both = dot1(rows_all[...], jnp.concatenate([gate_all[:, lanes], up_all[:, lanes]], axis=1))
        hidden[:, pl.ds(pl.multiple_of(i * 128, 128), 128)] = (silu(both[:, :128]) * both[:, 128:]).astype(BF16)
        return 0

    lax.fori_loop(0, many, ffn_in, 0)
    middle = sorted(range(ring), key=lambda q: abs(2 * q - ring + 1))
    order = [(q, 0) for q in middle] + [(q, 1) for q in middle]
    side = regions["L"][3]
    mids = regions["M"][3] - regions["M"][2]
    base = pl.multiple_of(first * 128, 128)
    f_sends = []

    def lanes_of(i):
        q, rel = order[i]
        s = q * 2 + (p if rel == 0 else 1 - p)
        return s, pl.ds(pl.multiple_of(s * dc, dc), dc)

    hop = 4 * own_rows

    def stage_a(i):
        q, rel = order[i]
        finish("D", q, rel)
        s, _ = lanes_of(i)

        @pl.when(has_m)
        def _():
            acc[i] = dot1(hidden[...], down_all[s, pl.ds(base, side + mids), :])

        @pl.when(jnp.logical_not(has_m))
        def _():
            acc[i] = dot1(hidden[:, :side], down_all[s, pl.ds(base, side), :])

        fd_send[i] = acc[i, pl.ds(pl.multiple_of((1 - c) * hop, hop), hop), :].astype(BF16)
        copy = remote(fd_send.at[i], fd_recv.at[i], fd_ssem.at[i], fd_rsem.at[i], sp, core)
        copy.start()
        f_sends.append(copy)

    def stage_b(i):
        f = remote(fd_send.at[i], fd_recv.at[i], fd_ssem.at[i], fd_rsem.at[i], sp, core)
        f.wait_recv()
        acc2[i] = acc[i, pl.ds(pl.multiple_of(c * hop, hop), hop), :] + fd_recv[i].astype(F32)
        fx_send[i] = acc2[i, pl.ds(pl.multiple_of((1 - x) * (hop // 2), hop // 2), hop // 2), :].astype(BF16)
        copy = remote(fx_send.at[i], fx_recv.at[i], fx_ssem.at[i], fx_rsem.at[i], sp, across)
        copy.start()
        f_sends.append(copy)

    def stage_c(i):
        f = remote(fx_send.at[i], fx_recv.at[i], fx_ssem.at[i], fx_rsem.at[i], sp, across)
        f.wait_recv()
        acc3[i] = acc2[i, pl.ds(pl.multiple_of(x * (hop // 2), hop // 2), hop // 2), :] + fx_recv[i].astype(F32)
        fz_send[i] = acc3[i, pl.ds(pl.multiple_of((1 - zz) * own_rows, own_rows), own_rows), :].astype(BF16)
        copy = remote(fz_send.at[i], fz_recv.at[i], fz_ssem.at[i], fz_rsem.at[i], mate, tp)
        copy.start()
        f_sends.append(copy)

    def stage_d(i):
        f = remote(fz_send.at[i], fz_recv.at[i], fz_ssem.at[i], fz_rsem.at[i], mate, tp)
        f.wait_recv()
        _, lanes = lanes_of(i)
        ffn = acc3[i, pl.ds(pl.multiple_of(zz * own_rows, own_rows), own_rows), :] + fz_recv[i].astype(F32)
        result[:, lanes] = (residual[:, lanes] + ffn).astype(BF16)

    ahead = {
        0: (("in", "H", 2), ("in", "L", 3), ("out", "L", 2), ("out", "H", 2)),
        2: (("in", "H", 3), ("out", "L", 3), ("out", "H", 3)),
    }
    for i in range(n + 5):
        for role, g, step in ahead.get(i, ()):
            relays("D", role, g, step)
        if i == 0:
            middles("D")
        if i < n:
            stage_a(i)
        if 0 <= i - 1 < n:
            stage_b(i - 1)
        if 0 <= i - 3 < n:
            stage_c(i - 3)
        if 0 <= i - 5 < n:
            stage_d(i - 5)

    for cond, make in sends:
        @pl.when(cond)
        def _():
            make().wait_send()
    for copy in [x_copy, w_x, w_d, w_xd] + [m for _, m in mix_copies] + t_copies + f_sends:
        copy.wait_send()
    assert max(len(taken["send"]), len(taken["recv"])) <= w_send.shape[0]


def paired_body(n, tps, stream, qp, kp, vp, gp, strength, decay_pre, extra, rate, head_gain, w_out,
                feed_gain, gate_m, up_m, down_m):
    heads, tokens = strength.shape
    own, width = stream.shape
    kr, units = gate_m.shape
    dc = down_m.shape[1]
    ring = n // 2
    side = (units // 128 - 1) // 2 * 128
    most = units - side
    group = 2 * tps * own
    dma = pltpu.SemaphoreType.DMA
    vmem = pl.BlockSpec(memory_space=pltpu.VMEM)
    hbm = pl.BlockSpec(memory_space=pl.ANY)
    count = 12 * ring
    return pl.pallas_call(
        functools.partial(paired_kernel, n, tps),
        out_shape=jax.ShapeDtypeStruct((own, width), BF16),
        in_specs=[vmem] * 11 + [hbm] * 4,
        out_specs=vmem,
        scratch_shapes=[
            pltpu.VMEM((kr * n, units), BF16),
            pltpu.VMEM((kr * n, units), BF16),
            pltpu.VMEM((n,) + down_m.shape, BF16),
            pltpu.VMEM((tps,) + w_out.shape, BF16),
            pltpu.VMEM((heads, tokens, 2 * HEAD), F32),
            pltpu.VMEM((heads, HEAD, 2 * HEAD), BF16),
            pltpu.VMEM((heads, HEAD, 2 * HEAD), BF16),
            pltpu.VMEM((heads, HEAD, 2 * HEAD), BF16),
            pltpu.VMEM((ring, heads, HEAD, 2 * HEAD), BF16),
            pltpu.VMEM((heads, HEAD, HEAD), F32),
            pltpu.VMEM((tokens, heads * HEAD), BF16),
            pltpu.VMEM((tps - 1, own, heads * HEAD), BF16),
            pltpu.VMEM((own, width), F32),
            pltpu.VMEM((group, width), BF16),
            pltpu.VMEM((group, most), BF16),
            pltpu.VMEM((n, group, dc), F32),
            pltpu.VMEM((n, group // 2, dc), F32),
            pltpu.VMEM((n, group // 4, dc), F32),
            pltpu.VMEM((n, group // 2, dc), BF16),
            pltpu.VMEM((n, group // 2, dc), BF16),
            pltpu.VMEM((n, group // 4, dc), BF16),
            pltpu.VMEM((n, group // 4, dc), BF16),
            pltpu.VMEM((n, group // 8, dc), BF16),
            pltpu.VMEM((n, group // 8, dc), BF16),
            dma((count,)), dma((count,)), dma((10,)), dma((2,)), dma((ring,)), dma((ring,)),
            dma((3,)), dma((3,)), dma((3,)), dma((3,)), dma((7,)), dma((7,)),
            dma((n,)), dma((n,)), dma((n,)), dma((n,)), dma((n,)), dma((n,)),
        ],
        compiler_params=pltpu.CompilerParams(
            collective_id=0, has_side_effects=True, vmem_limit_bytes=60 * 1024 * 1024),
    )(stream, qp, kp, vp, gp, strength, decay_pre, extra, rate[:, None], head_gain[None, :],
      feed_gain[None, :], w_out, gate_m, up_m, down_m)


def body(n, tps, *args):
    ring = n // 2
    short = ring % 4 == 0 and ring <= UNROLLED and tps == 4
    return (paired_body if short else chain_body)(n, tps, *args)


def solution(mesh):
    placed = (
        P(("sp", "tp"), None),
        P("sp", "tp"),
        P("sp", "tp"),
        P("sp", "tp"),
        P("sp", "tp"),
        P("tp", "sp"),
        P("tp", "sp"),
        P("tp", "sp"),
        P("tp"),
        P(),
        P("tp", None),
        P(),
        P("sp", "tp"),
        P("sp", "tp"),
        P("tp", "sp"),
    )
    return jax.shard_map(
        functools.partial(body, mesh.shape["sp"], mesh.shape["tp"]),
        mesh=mesh, in_specs=placed, out_specs=P(("sp", "tp"), None), check_vma=False,
    )
```

```python
import functools

import jax
import jax.numpy as jnp
from jax import lax
from jax.experimental import pallas as pl
from jax.experimental.pallas import tpu as pltpu
from jax.sharding import PartitionSpec as P

HEAD = 128
CHUNK = 128
UNROLLED = 4
EPSILON = 1e-06
F32 = jnp.float32
BF16 = jnp.bfloat16
HIGHEST = lax.Precision.HIGHEST
NN = (((1,), (0,)), ((), ()))
NT = (((1,), (1,)), ((), ()))
TN = (((0,), (0,)), ((), ()))


def dot1(a, b, dims=NN):
    return lax.dot_general(a, b, dims, preferred_element_type=F32)


def halves(x):
    high = x.astype(BF16)
    return high, (x - high.astype(F32)).astype(BF16)


def dot3(a, b, dims=NN):
    ah, al = halves(a)
    bh, bl = halves(b)
    return dot1(ah, bh, dims) + (dot1(ah, bl, dims) + dot1(al, bh, dims))


def silu(x):
    return x * jax.nn.sigmoid(x)


def local_scan(qp, kp, vp, strength, decay_pre, extra, rate, out_scr):
    heads, tokens = strength.shape
    chunks = tokens // CHUNK
    row_i = lax.broadcasted_iota(jnp.int32, (CHUNK, CHUNK), 0)
    col_i = lax.broadcasted_iota(jnp.int32, (CHUNK, CHUNK), 1)
    causal = row_i >= col_i
    strict = row_i > col_i
    eye = jnp.where(row_i == col_i, 1.0, 0.0).astype(F32)
    lower = jnp.where(causal, 1.0, 0.0).astype(F32)
    beta = jax.nn.sigmoid(strength[...].astype(F32))
    pre = decay_pre[...].astype(F32)
    soft = jnp.maximum(pre, 0.0) + jnp.log1p(jnp.exp(-jnp.abs(pre)))
    log_decay = -rate * soft + extra[...]

    pairs = [(h, c) for c in range(chunks) for h in range(heads)]
    data = {}
    for c in range(chunks):
        span = slice(c * CHUNK, (c + 1) * CHUNK)
        ld = log_decay[:, span]
        c_row = lax.dot_general(ld, lower, NT, precision=HIGHEST, preferred_element_type=F32)
        c_col = lax.dot_general(lower, ld, NT, precision=HIGHEST, preferred_element_type=F32)
        b_col = lax.dot_general(eye, beta[:, span], NT, precision=HIGHEST, preferred_element_type=F32)
        for h in range(heads):
            lanes = slice(h * HEAD, (h + 1) * HEAD)
            q = qp[span, lanes].astype(F32)
            k = kp[span, lanes].astype(F32)
            v = vp[span, lanes].astype(F32)
            q = q * (lax.rsqrt(jnp.sum(q * q, axis=-1, keepdims=True) + EPSILON) * HEAD ** (-0.5))
            k = k * lax.rsqrt(jnp.sum(k * k, axis=-1, keepdims=True) + EPSILON)
            cc = c_col[:, h:h + 1]
            bb = b_col[:, h:h + 1]
            cr = c_row[h:h + 1, :]
            last = cr[:, CHUNK - 1:]
            damp = jnp.where(causal, jnp.exp(jnp.where(causal, cc - cr, 0.0)), 0.0)
            grown = jnp.exp(cc)
            kb = k * bb
            kk = dot3(kb, k, NT) * jnp.where(strict, damp, 0.0)
            inner = dot3(q, k, NT) * damp
            data[h, c] = dict(
                low=kk, inner=inner, v=v * bb, kw=kb * grown, qd=q * grown,
                kd=k * jnp.exp(last - cc), decay=jnp.exp(last),
            )
    inverse = {}
    b = 1
    shift = 0
    while b < CHUNK:
        mask = ((row_i >> (shift + 1)) == (col_i >> (shift + 1))) & (
            ((row_i >> shift) & 1) == 1) & (((col_i >> shift) & 1) == 0)
        for key in pairs:
            piece = jnp.where(mask, data[key]["low"], 0.0)
            if b == 1:
                inverse[key] = eye - piece
            else:
                x = inverse[key]
                inverse[key] = x - dot3(x, dot3(piece, x))
        b *= 2
        shift += 1
    states = [jnp.concatenate([jnp.zeros((HEAD, HEAD), F32), eye], axis=1) for _ in range(heads)]
    for c in range(chunks):
        for h in range(heads):
            e = data[h, c]
            u = dot3(inverse[h, c], e["v"])
            w = dot3(inverse[h, c], e["kw"])
            x = states[h]
            new = jnp.concatenate([u, jnp.zeros_like(u)], axis=1) - dot3(w, x)
            out_scr[h, c * CHUNK:(c + 1) * CHUNK, :] = dot3(e["qd"], x) + dot3(e["inner"], new)
            states[h] = e["decay"] * x + dot3(e["kd"], new, TN)
    return states


def combine(states, x_part, p, p_send):
    heads = len(states)
    for h in range(heads):
        mine = states[h]
        theirs = x_part[h].astype(F32)
        before = jnp.where(p == 0, mine, theirs)
        after = jnp.where(p == 0, theirs, mine)
        after_s = jnp.concatenate([after[:, :HEAD], jnp.zeros((HEAD, HEAD), F32)], axis=1)
        p_send[h] = (dot3(after[:, HEAD:], before) + after_s).astype(BF16)


def fold_states(r, p_recv, s_in, heads):
    s_in[...] = jnp.zeros_like(s_in)

    def fold(i, _):
        for h in range(heads):
            got = p_recv[i, h].astype(F32)
            s_in[h] = dot3(got[:, HEAD:], s_in[h]) + got[:, :HEAD]
        return 0

    lax.fori_loop(0, r, fold, 0)


def apply_state(p, x_part, s_in, out_scr, head_gain, gp, mixed, heads):
    for h in range(heads):
        lanes = slice(h * HEAD, (h + 1) * HEAD)
        got = x_part[h].astype(F32)
        s = s_in[h]
        s = jnp.where(p == 0, s, dot3(got[:, HEAD:], s) + got[:, :HEAD])
        att = out_scr[h, :, :HEAD] + dot3(out_scr[h, :, HEAD:], s)
        att = att * lax.rsqrt(jnp.mean(att * att, axis=-1, keepdims=True) + EPSILON) * head_gain[...]
        mixed[:, lanes] = (att * silu(gp[:, lanes].astype(F32))).astype(BF16)


def messages(ring):
    own_z = [(a, 0, 0, way) for a in "GU" for way in "RL"]
    own_y = [(a, 0, 0, "Y") for a in "GU"]
    first = own_z + own_y
    down_y = [("D", 0, 0, "Y")]

    def relay(a, j, skip_y=False):
        out = []
        if j < ring - 1:
            out += [(a, -j, 0, "R"), (a, j, 0, "L")]
        if not skip_y:
            out += [(a, -j, 0, "Y"), (a, j, 0, "Y")]
        return out

    early, middle, later, last = [], [], [], []
    if ring > 1:
        early = relay("G", 1)
        middle = relay("U", 1)
        for j in range(2, ring):
            later += relay("G", j) + relay("U", j)
            if j == 2:
                later += [("D", 0, 0, "R"), ("D", 0, 0, "L")]
        if ring == 2:
            later += [("D", 0, 0, "R"), ("D", 0, 0, "L")]
        later += [("D", 0, 1, "R"), ("D", 0, 1, "L")]
        later += relay("D", 1, skip_y=True)
        for j in range(2, ring):
            last += relay("D", j)
    else:
        first = own_y
    return first, down_y, early, middle, later, last


def chain_kernel(
    n, tps, groups,
    stream, qp, kp, vp, gp, strength, decay_pre, extra, rate, head_gain, w_out, feed_gain,
    gate_in, up_in, down_in,
    result,
    gate_all, up_all, down_all, out_scr, x_send, x_part, p_send, p_recv, s_in, mixed,
    d_send, d_recv, residual, rows_all, hidden, f_part, f_recv,
    w_send, w_recv, own_sem, x_sem, p_ssem, p_rsem, d_ssem, d_rsem, e_ssem, e_rsem, f_ssem, f_rsem,
):
    ring = n // 2
    sp = lax.axis_index("sp")
    tp = lax.axis_index("tp")
    r = sp // 2
    p = lax.rem(sp, 2)
    heads = strength.shape[0]
    tokens = strength.shape[1]
    chunks = tokens // CHUNK
    own_rows = stream.shape[0]
    kr = gate_in.shape[0]
    MESH = pl.DeviceIdType.MESH

    def sp_of(dr, rel):
        q = p if rel == 0 else 1 - p
        return lax.rem(r + dr + ring, ring) * 2 + q

    partner = sp_of(0, 1)
    where = {"R": sp_of(1, 0), "L": sp_of(-1, 0), "Y": partner}

    def tp_peer(o):
        return lax.rem(tp + o, tps)

    barrier = pltpu.get_barrier_semaphore()
    for dr in range(1, ring):
        pl.semaphore_signal(barrier, 1, device_id=(sp_of(dr, 0), tp), device_id_type=MESH)
    pl.semaphore_signal(barrier, 1, device_id=(partner, tp), device_id_type=MESH)
    for o in range(1, tps):
        pl.semaphore_signal(barrier, 1, device_id=(sp, tp_peer(o)), device_id_type=MESH)
    pl.semaphore_wait(barrier, ring + tps - 1)

    flat = [m for g in groups for m in g]
    number = {m: i for i, m in enumerate(flat)}
    arrival = {}
    for (a, dr, rel, way) in flat:
        to = {"R": (dr - 1, rel), "L": (dr + 1, rel), "Y": (dr, 1 - rel)}[way]
        key = (a, to[0], to[1])
        assert key not in arrival
        arrival[key] = number[(a, dr, rel, way)]
    waited = set()
    copies = []

    def exists(dr):
        return (r + dr >= 0) & (r + dr < ring)

    def slot(a, dr, rel):
        s = sp_of(dr, rel)
        if a == "D":
            return down_all.at[s]
        whole = gate_all if a == "G" else up_all
        return whole.at[pl.ds(pl.multiple_of(s * kr, kr), kr), :]

    inputs = {"G": gate_in, "U": up_in, "D": down_in}

    def need(a, dr, rel):
        key = (a, dr, rel)
        if (dr == 0 and rel == 0) or key in waited:
            return
        waited.add(key)
        m = arrival[key]

        @pl.when(exists(dr))
        def _():
            here = slot(*key)
            pltpu.make_async_remote_copy(
                here, here, w_send.at[m], w_recv.at[m], device_id=(partner, tp), device_id_type=MESH
            ).wait_recv()

    def outgoing(message):
        a, dr, rel, way = message
        m = number[message]
        return pltpu.make_async_remote_copy(
            inputs[a] if dr == 0 and rel == 0 else slot(a, dr, rel),
            slot(a, dr, rel),
            w_send.at[m], w_recv.at[m],
            device_id=(where[way], tp), device_id_type=MESH,
        )

    def goes(message):
        ahead = {"R": r + 1 < ring, "L": r >= 1, "Y": r >= 0}[message[3]]
        return exists(message[1]) & ahead

    def pump(group):
        for message in group:
            need(*message[:3])

            @pl.when(goes(message))
            def _():
                outgoing(message).start()

            copies.append(message)

    def need_all(a):
        for dr in sorted(range(1 - ring, ring), key=abs):
            for rel in (0, 1):
                need(a, dr, rel)

    first, down_y, early, middle, later, last_group = groups
    pump(first)
    locals_ = []
    for i, a in enumerate("GUD"):
        local = pltpu.make_async_copy(inputs[a], slot(a, 0, 0), own_sem.at[i])
        local.start()
        locals_.append(local)

    states = local_scan(qp, kp, vp, strength, decay_pre, extra, rate[...], out_scr)
    for h in range(heads):
        x_send[h] = states[h].astype(BF16)
    x_copy = pltpu.make_async_remote_copy(
        x_send, x_part, x_sem.at[0], x_sem.at[1], device_id=(partner, tp), device_id_type=MESH)
    x_copy.start()
    pump(down_y)
    x_copy.wait_recv()
    combine(states, x_part, p, p_send)

    def p_copy(k, to, at):
        return pltpu.make_async_remote_copy(
            p_send, p_recv.at[at], p_ssem.at[k], p_rsem.at[k],
            device_id=(to, tp), device_id_type=MESH)

    for k in range(1, ring):
        @pl.when(r + k < ring)
        def _():
            p_copy(k, sp_of(k, 0), r).start()
    pump(early)
    for k in range(1, ring):
        @pl.when(r - k >= 0)
        def _():
            p_copy(k, sp_of(-k, 0), r - k).wait_recv()
    fold_states(r, p_recv, s_in, heads)
    apply_state(p, x_part, s_in, out_scr, head_gain, gp, mixed, heads)

    def rows_of(t):
        return pl.ds(pl.multiple_of(t * own_rows, own_rows), own_rows)

    order = [o for o in (2, 3, 1) if o < tps] + list(range(4, tps))
    d_copies = []
    for o in order:
        to = tp_peer(o)
        d_send[o - 1] = dot1(mixed[rows_of(to), :], w_out[...]).astype(BF16)
        copy = pltpu.make_async_remote_copy(
            d_send.at[o - 1], d_recv.at[o - 1], d_ssem.at[o - 1], d_rsem.at[o - 1],
            device_id=(sp, to), device_id_type=MESH)
        copy.start()
        d_copies.append(copy)
    pump(middle)
    total = dot1(mixed[rows_of(tp), :], w_out[...]).astype(BF16).astype(F32)
    for copy in d_copies:
        copy.wait_recv()
    for o in range(1, tps):
        total = total + d_recv[o - 1].astype(F32)
    total = stream[...].astype(F32) + total
    residual[...] = total
    rows_all[rows_of(tp), :] = (
        total * lax.rsqrt(jnp.mean(total * total, axis=-1, keepdims=True) + EPSILON) * feed_gain[...]
    ).astype(BF16)
    e_copies = []
    for o in order:
        copy = pltpu.make_async_remote_copy(
            rows_all.at[rows_of(tp), :], rows_all.at[rows_of(tp), :], e_ssem.at[o - 1], e_rsem.at[o - 1],
            device_id=(sp, tp_peer(o)), device_id_type=MESH)
        copy.start()
        e_copies.append(copy)
    for o in order:
        there = rows_all.at[rows_of(lax.rem(tp - o + tps, tps)), :]
        pltpu.make_async_remote_copy(
            there, there, e_ssem.at[o - 1], e_rsem.at[o - 1],
            device_id=(sp, tp_peer(o)), device_id_type=MESH).wait_recv()
    pump(later)
    need_all("G")
    need_all("U")
    for local in locals_:
        local.wait()

    tile = 128

    def ffn_in(i, _):
        lanes = pl.ds(pl.multiple_of(i * tile, tile), tile)
        both = dot1(rows_all[...], jnp.concatenate([gate_all[:, lanes], up_all[:, lanes]], axis=1))
        hidden[:, lanes] = (silu(both[:, :tile]) * both[:, tile:]).astype(BF16)
        return 0

    lax.fori_loop(0, gate_all.shape[1] // tile, ffn_in, 0)
    pump(last_group)
    need_all("D")
    dc = down_all.shape[2]
    pack = max(1, 128 // dc)
    wide = pack * dc

    def ffn_out(i, _):
        lanes = pl.ds(pl.multiple_of(i * wide, wide), wide)
        if pack == 1:
            weights = down_all[i]
        else:
            weights = jnp.concatenate([down_all[i * pack + j] for j in range(pack)], axis=1)
        f_part[:, lanes] = dot1(hidden[...], weights).astype(BF16)
        return 0

    lax.fori_loop(0, n // pack, ffn_out, 0)
    f_copies = []
    for o in order:
        copy = pltpu.make_async_remote_copy(
            f_part.at[rows_of(tp_peer(o)), :], f_recv.at[o - 1], f_ssem.at[o - 1], f_rsem.at[o - 1],
            device_id=(sp, tp_peer(o)), device_id_type=MESH)
        copy.start()
        f_copies.append(copy)
    ffn = f_part[rows_of(tp), :].astype(F32)
    for copy in f_copies:
        copy.wait_recv()
    for o in range(1, tps):
        ffn = ffn + f_recv[o - 1].astype(F32)
    result[...] = (residual[...] + ffn).astype(BF16)

    for message in copies:
        @pl.when(goes(message))
        def _():
            outgoing(message).wait_send()
    for copy in [x_copy] + d_copies + e_copies + f_copies:
        copy.wait_send()
    for k in range(1, ring):
        @pl.when(r + k < ring)
        def _():
            p_copy(k, sp_of(k, 0), r).wait_send()


def chain_body(n, tps, stream, qp, kp, vp, gp, strength, decay_pre, extra, rate, head_gain, w_out,
         feed_gain, gate_m, up_m, down_m):
    heads, tokens = strength.shape
    own, width = stream.shape
    kr, units = gate_m.shape
    ring = n // 2
    groups = messages(ring)
    count = sum(len(g) for g in groups)
    dma = pltpu.SemaphoreType.DMA
    vmem = pl.BlockSpec(memory_space=pltpu.VMEM)
    hbm = pl.BlockSpec(memory_space=pl.ANY)
    peers = max(1, tps - 1)
    return pl.pallas_call(
        functools.partial(chain_kernel, n, tps, groups),
        out_shape=jax.ShapeDtypeStruct((own, width), BF16),
        in_specs=[vmem] * 12 + [hbm] * 3,
        out_specs=vmem,
        scratch_shapes=[
            pltpu.VMEM((kr * n, units), BF16),
            pltpu.VMEM((kr * n, units), BF16),
            pltpu.VMEM((n,) + down_m.shape, BF16),
            pltpu.VMEM((heads, tokens, 2 * HEAD), F32),
            pltpu.VMEM((heads, HEAD, 2 * HEAD), BF16),
            pltpu.VMEM((heads, HEAD, 2 * HEAD), BF16),
            pltpu.VMEM((heads, HEAD, 2 * HEAD), BF16),
            pltpu.VMEM((ring, heads, HEAD, 2 * HEAD), BF16),
            pltpu.VMEM((heads, HEAD, HEAD), F32),
            pltpu.VMEM((tokens, heads * HEAD), BF16),
            pltpu.VMEM((peers, own, width), BF16),
            pltpu.VMEM((peers, own, width), BF16),
            pltpu.VMEM((own, width), F32),
            pltpu.VMEM((tokens, width), BF16),
            pltpu.VMEM((tokens, units), BF16),
            pltpu.VMEM((tokens, width), BF16),
            pltpu.VMEM((peers, own, width), BF16),
            dma((count,)), dma((count,)), dma((3,)), dma((2,)), dma((ring,)), dma((ring,)),
            dma((peers,)), dma((peers,)), dma((peers,)), dma((peers,)), dma((peers,)), dma((peers,)),
        ],
        compiler_params=pltpu.CompilerParams(
            collective_id=0, has_side_effects=True, vmem_limit_bytes=60 * 1024 * 1024),
    )(stream, qp, kp, vp, gp, strength, decay_pre, extra, rate[:, None], head_gain[None, :], w_out,
      feed_gain[None, :], gate_m, up_m, down_m)


def regions_of(ring, units):
    tiles = units // 128
    side = (tiles - 1) // 2 * 128
    half, quarter = ring // 2, ring // 4
    return {
        "L": (0, half, 0, side),
        "M": (quarter, half + quarter, side, units - side),
        "H": (half, ring, units - side, units),
    }


def paired_kernel(
    n, tps,
    stream_in, qp_in, kp_in, vp_in, gp_in, strength_in, decay_in, extra_in, rate_in, head_gain_in, feed_gain_in,
    w_out, gate_in, up_in, down_in,
    result,
    stream, qp, kp, vp, gp, strength, decay_pre, extra, rate, head_gain, feed_gain, in_sem,
    gate_all, up_all, down_all, w_all, out_scr, x_send, x_part, p_send, s_send, s_got, s_in, mixed, mix_all,
    residual, rows_all, hidden, acc, acc2, acc3, fd_send, fd_recv, fx_send, fx_recv, fz_send, fz_recv,
    w_send, w_recv, own_sem, x_sem, s_sem, wo_ssem, wo_rsem, m_ssem, m_rsem, t_ssem, t_rsem,
    fd_ssem, fd_rsem, fx_ssem, fx_rsem, fz_ssem, fz_rsem,
):
    loads = []
    for i, (src, dst) in enumerate((
        (strength_in, strength), (decay_in, decay_pre), (extra_in, extra), (rate_in, rate), (kp_in, kp), (qp_in, qp),
        (vp_in, vp), (gp_in, gp), (stream_in, stream), (head_gain_in, head_gain), (feed_gain_in, feed_gain),
    )):
        load = pltpu.make_async_copy(src, dst, in_sem.at[i])
        load.start()
        loads.append(load)
    ring = n // 2
    half = ring // 2
    sp = lax.axis_index("sp")
    tp = lax.axis_index("tp")
    r = sp // 2
    p = lax.rem(sp, 2)
    x = tp // 2
    c = lax.rem(tp, 2)
    zz = jnp.where(r >= half, 1, 0)
    heads = strength.shape[0]
    own_rows = stream.shape[0]
    kr, units = gate_in.shape
    width = stream.shape[1]
    dc = down_in.shape[1]
    MESH = pl.DeviceIdType.MESH
    regions = regions_of(ring, units)
    partner = r * 2 + 1 - p
    mate = lax.rem(r + half, ring) * 2 + p
    core = x * 2 + 1 - c
    across = (1 - x) * 2 + c
    diagonal = (1 - x) * 2 + 1 - c

    def at(q):
        return q * 2 + p

    def remote(src, dst, ssem, rsem, sp_to, tp_to):
        return pltpu.make_async_remote_copy(src, dst, ssem, rsem, device_id=(sp_to, tp_to), device_id_type=MESH)

    inputs = {"G": gate_in, "U": up_in, "D": down_in}
    def spans(g, k):
        return (k >= regions[g][0]) & (k < regions[g][1])

    taken = {"send": [], "recv": []}

    def color(kind, users):
        for i, held in enumerate(taken[kind]):
            if not held & users:
                held |= users
                return i
        taken[kind].append(set(users))
        return len(taken[kind]) - 1

    number = {}
    for a in "GUD":
        for g in "LMH":
            for q in range(ring):
                for rel in (0, 1):
                    users = {k for k in range(ring) if spans(g, k) and (rel == 1 or k != q)}
                    number[a, g, q, rel] = color("recv", users)

    def slot(a, g, q, rel):
        s = q * 2 + (p if rel == 0 else 1 - p)
        c0, c1 = regions[g][2:]
        if a == "D":
            return down_all.at[s, c0:c1, :]
        whole = gate_all if a == "G" else up_all
        return whole.at[pl.ds(pl.multiple_of(s * kr, kr), kr), c0:c1]

    def own(a, g):
        c0, c1 = regions[g][2:]
        return inputs[a].at[c0:c1, :] if a == "D" else inputs[a].at[:, c0:c1]

    def member(g):
        return spans(g, r)

    own_copies = []
    for i, a in enumerate("GUD"):
        for j, g in enumerate("LMH"):
            for q in range(*regions[g][:2]):
                copy = pltpu.make_async_copy(own(a, g), slot(a, g, q, 0), own_sem.at[3 * i + j])
                own_copies.append((r == q, copy))

                @pl.when(r == q)
                def _():
                    copy.start()

    w_local = pltpu.make_async_copy(w_out, w_all.at[tp], own_sem.at[9])
    w_local.start()

    barrier = pltpu.get_barrier_semaphore()
    for k in range(1, ring):
        pl.semaphore_signal(barrier, 1, device_id=(at(lax.rem(r + k, ring)), tp), device_id_type=MESH)
    pl.semaphore_signal(barrier, 1, device_id=(partner, tp), device_id_type=MESH)
    for k in range(1, tps):
        pl.semaphore_signal(barrier, 1, device_id=(sp, lax.rem(tp + k, tps)), device_id_type=MESH)
    pl.semaphore_wait(barrier, ring + tps - 1)

    def detour(a, g, q, to):
        lo, hi = regions[g][:2]
        if g == "M" or hi - lo < 2:
            return False
        inner, outer = (hi - 1, hi - 2) if g == "L" else (lo, lo + 1)
        return a != "G" and (q, to) == (outer, inner)

    sends = []
    waited = set()

    def send(cond, src, key, way, sp_to):
        users = {k for k in range(ring) if cond(k)}
        if not users:
            return
        m = color("send", users)
        landing = key[:3] + (1,) if way == "y" else key

        def make():
            return remote(src, slot(*key), w_send.at[m], w_recv.at[number[landing]], sp_to, tp)

        @pl.when(cond(r))
        def _():
            make().start()

        sends.append((cond(r), make))

    def forwards_y(a, g, q, k):
        return spans(g, k) and not detour(a, g, q, k)

    def own_sends(a, ways, only=None):
        for g in "LMH":
            lo, hi = regions[g][:2]
            for q in range(ring):
                if only is not None and q not in only:
                    continue
                key = (a, g, q, 0)
                mine = functools.partial(lambda q, k: k == q, q)
                inside = lo <= q < hi
                here = slot(*key) if inside else own(a, g)
                if inside and "y" in ways:
                    send(mine, here, key, "y", partner)
                if g == "M":
                    targets = [to for to in range(lo, hi) if to != q]
                elif inside:
                    targets = [to for to in (q - 1, q + 1) if lo <= to < hi]
                else:
                    targets = [lo if q < lo else hi - 1]
                for to in targets:
                    way = "l" if to < q else "r"
                    if (way if abs(q - to) == 1 else way.upper()) in ways:
                        send(mine, here, key, way, at(to))

    def arrived(key, cond):
        here = slot(*key)

        @pl.when(cond)
        def _():
            remote(here, here, w_send.at[0], w_recv.at[number[key]], partner, tp).wait_recv()

    def role_of(g, role, k):
        lo, hi = regions[g][:2]
        inner = hi - 1 if g == "L" else lo
        return True if role is None else (k == inner) if role == "in" else (k != inner)

    def relay(a, g, q, role):
        key = (a, g, q, 0)
        lo, hi = regions[g][:2]
        assert (key, role) not in waited
        waited.add((key, role))

        def holds(k):
            return spans(g, k) & (k != q) & role_of(g, role, k)

        if any(holds(k) for k in range(ring)):
            arrived(key, holds(r))
        here = slot(*key)
        if g != "M":
            send(lambda k: holds(k) & (k > lo) & (k < q), here, key, "l", at(r - 1))
            send(lambda k: holds(k) & (k > q) & (k < hi - 1), here, key, "r", at(r + 1))
        for k in range(lo, hi):
            if holds(k) and forwards_y(a, g, q, k):
                send(functools.partial(lambda k, kk: kk == k, k), here, key, "y", partner)

    def detours(a):
        for g in "LH":
            for q in range(*regions[g][:2]):
                for to in (q - 1, q + 1):
                    if detour(a, g, q, to):
                        key = (a, g, q, 1)
                        arrived(key, r == q)
                        early.setdefault(key, []).append(q)
                        send(functools.partial(lambda q, k: k == q, q), slot(*key), key, "z", at(to))

    early = {}
    low = list(range(half - 1, -1, -1)) + list(range(half, ring))

    def relays(a, role, g, *steps):
        for i in steps:
            relay(a, g, low[i] if g == "L" else ring - 1 - low[i], role)

    def middles(a):
        for q in range(ring):
            relay(a, "M", q, None)

    def finish(a, q, rel):
        for g in "LMH":
            key = (a, g, q, rel)
            if rel == 1:
                cond = member(g)
                for done in early.get(key, []):
                    cond = cond & (r != done)
                arrived(key, cond)
                continue
            for role in (None,) if g == "M" else ("in", "out"):
                if (key, role) not in waited:
                    waited.add((key, role))
                    mine = member(g) & (r != q)
                    arrived(key, mine & role_of(g, role, r))

    for cond, copy in own_copies:
        @pl.when(cond)
        def _():
            copy.wait()
    own_sends("G", "LR")
    own_sends("G", "ly")
    own_sends("G", "r", range(1, ring))
    w_local.wait()
    w_x = remote(w_all.at[tp], w_all.at[tp], wo_ssem.at[0], wo_rsem.at[0], sp, across)
    w_half = w_out.shape[0] // 2
    w_part = w_all.at[tp, :w_half, :]
    remote(w_part, w_part, wo_ssem.at[0], wo_rsem.at[0], sp, across).start()
    w_d = remote(w_all.at[tp], w_all.at[tp], wo_ssem.at[1], wo_rsem.at[1], sp, core)
    w_d.start()
    w_xd = remote(w_all.at[across], w_all.at[across], wo_ssem.at[2], wo_rsem.at[2], sp, core)

    for load in loads:
        load.wait()
    square = (heads, heads)
    same = lax.broadcasted_iota(jnp.int32, square, 0) == lax.broadcasted_iota(jnp.int32, square, 1)
    rates = jnp.sum(jnp.where(same, jnp.broadcast_to(rate[...], square), 0.0), axis=1, keepdims=True)
    states = local_scan(qp, kp, vp, strength, decay_pre, extra, rates, out_scr)
    for h in range(heads):
        x_send[h] = states[h].astype(BF16)
    x_copy = remote(x_send, x_part, x_sem.at[0], x_sem.at[1], partner, tp)
    x_copy.start()
    own_sends("U", "lL")
    own_sends("U", "r", range(half, ring))
    x_copy.wait_recv()
    combine(states, x_part, p, p_send)

    def s_copy(src, to):
        return remote(src, s_got, s_sem.at[0], s_sem.at[1], at(to), tp)

    s_in[...] = jnp.zeros_like(s_in)

    @pl.when(r == 0)
    def _():
        s_copy(p_send.at[:, :, :HEAD], 1).start()

    own_sends("G", "r", range(1))
    w_rest = w_all.at[tp, w_half:, :]
    remote(w_rest, w_rest, wo_ssem.at[0], wo_rsem.at[0], sp, across).start()
    own_sends("U", "y")
    relays("G", "out", "L", 0)
    relays("G", "out", "H", 0)
    relays("G", "in", "H", 1)

    @pl.when(r > 0)
    def _():
        s_copy(s_send, 0).wait_recv()
        for h in range(heads):
            s_in[h] = s_got[h].astype(F32)

    @pl.when((r > 0) & (r + 1 < ring))
    def _():
        for h in range(heads):
            both = p_send[h].astype(F32)
            s_send[h] = (dot3(both[:, HEAD:], s_in[h]) + both[:, :HEAD]).astype(BF16)
        s_copy(s_send, lax.rem(r + 1, ring)).start()

    own_sends("U", "r", range(1, half))
    relays("G", "in", "L", 2, 3)
    own_sends("D", "y")
    w_x.wait_recv()
    w_xd.start()
    own_sends("U", "R")
    apply_state(p, x_part, s_in, out_scr, head_gain, gp, mixed, heads)

    def token_rows(t):
        return pl.ds(pl.multiple_of(t * own_rows, own_rows), own_rows)

    mix_copies = []
    for i, to in enumerate((across, diagonal, core)):
        copy = remote(mixed.at[token_rows(to), :], mix_all.at[i], m_ssem.at[i], m_rsem.at[i], sp, to)
        copy.start()
        mix_copies.append((to, copy))
    relays("G", "in", "H", 2, 3)
    relays("G", "in", "L", 1)
    relays("G", "out", "L", 2)
    relays("U", "out", "L", 0)
    total = dot1(mixed[token_rows(tp), :], w_all[tp]).astype(BF16).astype(F32)
    w_d.wait_recv()
    w_xd.wait_recv()
    for i, (to, copy) in enumerate(mix_copies):
        copy.wait_recv()
        total = total + dot1(mix_all[i], w_all[to]).astype(BF16).astype(F32)
    total = stream[...].astype(F32) + total
    residual[...] = total
    normed = (
        total * lax.rsqrt(jnp.mean(total * total, axis=-1, keepdims=True) + EPSILON) * feed_gain[...]
    ).astype(BF16)

    def block_of(z_, x_, c_):
        b = (c_ * 2 + x_) * 2 + z_
        return rows_all.at[pl.ds(pl.multiple_of(b * own_rows, own_rows), own_rows), :]

    b_own = (c * 2 + x) * 2 + zz
    rows_all[pl.ds(pl.multiple_of(b_own * own_rows, own_rows), own_rows), :] = normed
    t_copies = []

    def token(i, block, sp_to, tp_to):
        copy = remote(block, block, t_ssem.at[i], t_rsem.at[i], sp_to, tp_to)
        copy.start()
        t_copies.append(copy)

    def token_wait(i, block):
        remote(block, block, t_ssem.at[i], t_rsem.at[i], sp, across).wait_recv()

    token(0, block_of(zz, x, c), mate, tp)
    token(1, block_of(zz, x, c), sp, across)
    token(2, block_of(zz, x, c), sp, core)
    own_sends("U", "r", range(1))
    relays("G", "out", "L", 3)
    relays("G", "out", "H", 2)
    relays("U", "in", "L", 2)
    relays("U", "in", "H", 1)
    relays("U", "out", "H", 0)
    middles("G")
    detours("U")
    relays("U", "in", "L", 3)
    token_wait(1, block_of(zz, 1 - x, c))
    token(5, block_of(zz, 1 - x, c), sp, core)
    relays("G", "out", "H", 3)
    relays("U", "in", "H", 2, 3)
    own_sends("D", "lr")
    relays("U", "out", "L", 2)
    relays("U", "out", "H", 2)
    own_sends("D", "LR")
    relays("U", "in", "L", 1)
    relays("U", "out", "L", 3)
    relays("U", "out", "H", 3)
    token_wait(0, block_of(1 - zz, x, c))
    token(3, block_of(1 - zz, x, c), sp, across)
    token(4, block_of(1 - zz, x, c), sp, core)
    middles("U")
    token_wait(3, block_of(1 - zz, 1 - x, c))
    token(6, block_of(1 - zz, 1 - x, c), sp, core)
    relays("D", "out", "L", 0)
    relays("D", "out", "H", 0)
    relays("D", "in", "L", 1, 2)
    relays("D", "in", "H", 1)
    detours("D")
    relays("D", "in", "H", 2)
    relays("D", "in", "L", 3)
    relays("D", "in", "H", 3)
    token_wait(2, block_of(zz, x, 1 - c))
    token_wait(4, block_of(1 - zz, x, 1 - c))
    token_wait(5, block_of(zz, 1 - x, 1 - c))
    token_wait(6, block_of(1 - zz, 1 - x, 1 - c))
    for a in "GU":
        for rel in (0, 1):
            for q in range(ring):
                finish(a, q, rel)

    has_m = member("M")
    first = jnp.where(r < half, 0, jnp.where(has_m, regions["M"][2] // 128, regions["H"][2] // 128))
    many = (regions["L"][3] - regions["L"][2]) // 128 + jnp.where(has_m, (regions["M"][3] - regions["M"][2]) // 128, 0)

    def ffn_in(i, _):
        lanes = pl.ds(pl.multiple_of((first + i) * 128, 128), 128)
        both = dot1(rows_all[...], jnp.concatenate([gate_all[:, lanes], up_all[:, lanes]], axis=1))
        hidden[:, pl.ds(pl.multiple_of(i * 128, 128), 128)] = (silu(both[:, :128]) * both[:, 128:]).astype(BF16)
        return 0

    lax.fori_loop(0, many, ffn_in, 0)
    middle = sorted(range(ring), key=lambda q: abs(2 * q - ring + 1))
    order = [(q, 0) for q in middle] + [(q, 1) for q in middle]
    side = regions["L"][3]
    mids = regions["M"][3] - regions["M"][2]
    base = pl.multiple_of(first * 128, 128)
    f_sends = []

    def lanes_of(i):
        q, rel = order[i]
        s = q * 2 + (p if rel == 0 else 1 - p)
        return s, pl.ds(pl.multiple_of(s * dc, dc), dc)

    hop = 4 * own_rows

    def stage_a(i):
        q, rel = order[i]
        finish("D", q, rel)
        s, _ = lanes_of(i)

        @pl.when(has_m)
        def _():
            acc[i] = dot1(hidden[...], down_all[s, pl.ds(base, side + mids), :])

        @pl.when(jnp.logical_not(has_m))
        def _():
            acc[i] = dot1(hidden[:, :side], down_all[s, pl.ds(base, side), :])

        fd_send[i] = acc[i, pl.ds(pl.multiple_of((1 - c) * hop, hop), hop), :].astype(BF16)
        copy = remote(fd_send.at[i], fd_recv.at[i], fd_ssem.at[i], fd_rsem.at[i], sp, core)
        copy.start()
        f_sends.append(copy)

    def stage_b(i):
        f = remote(fd_send.at[i], fd_recv.at[i], fd_ssem.at[i], fd_rsem.at[i], sp, core)
        f.wait_recv()
        acc2[i] = acc[i, pl.ds(pl.multiple_of(c * hop, hop), hop), :] + fd_recv[i].astype(F32)
        fx_send[i] = acc2[i, pl.ds(pl.multiple_of((1 - x) * (hop // 2), hop // 2), hop // 2), :].astype(BF16)
        copy = remote(fx_send.at[i], fx_recv.at[i], fx_ssem.at[i], fx_rsem.at[i], sp, across)
        copy.start()
        f_sends.append(copy)

    def stage_c(i):
        f = remote(fx_send.at[i], fx_recv.at[i], fx_ssem.at[i], fx_rsem.at[i], sp, across)
        f.wait_recv()
        acc3[i] = acc2[i, pl.ds(pl.multiple_of(x * (hop // 2), hop // 2), hop // 2), :] + fx_recv[i].astype(F32)
        fz_send[i] = acc3[i, pl.ds(pl.multiple_of((1 - zz) * own_rows, own_rows), own_rows), :].astype(BF16)
        copy = remote(fz_send.at[i], fz_recv.at[i], fz_ssem.at[i], fz_rsem.at[i], mate, tp)
        copy.start()
        f_sends.append(copy)

    def stage_d(i):
        f = remote(fz_send.at[i], fz_recv.at[i], fz_ssem.at[i], fz_rsem.at[i], mate, tp)
        f.wait_recv()
        _, lanes = lanes_of(i)
        ffn = acc3[i, pl.ds(pl.multiple_of(zz * own_rows, own_rows), own_rows), :] + fz_recv[i].astype(F32)
        result[:, lanes] = (residual[:, lanes] + ffn).astype(BF16)

    ahead = {
        0: (("out", "L", 2), ("out", "H", 2)),
        2: (("out", "L", 3), ("out", "H", 3)),
    }
    for i in range(n + 5):
        for role, g, step in ahead.get(i, ()):
            relays("D", role, g, step)
        if i == 0:
            middles("D")
        if i < n:
            stage_a(i)
        if 0 <= i - 1 < n:
            stage_b(i - 1)
        if 0 <= i - 3 < n:
            stage_c(i - 3)
        if 0 <= i - 5 < n:
            stage_d(i - 5)

    for cond, make in sends:
        @pl.when(cond)
        def _():
            make().wait_send()
    for copy in [x_copy, w_x, w_d, w_xd] + [m for _, m in mix_copies] + t_copies + f_sends:
        copy.wait_send()

    @pl.when(r == 0)
    def _():
        s_copy(p_send.at[:, :, :HEAD], 1).wait_send()

    @pl.when((r > 0) & (r + 1 < ring))
    def _():
        s_copy(s_send, 0).wait_send()

    assert max(len(taken["send"]), len(taken["recv"])) <= w_send.shape[0]


def paired_body(n, tps, stream, qp, kp, vp, gp, strength, decay_pre, extra, rate, head_gain, w_out,
                feed_gain, gate_m, up_m, down_m):
    heads, tokens = strength.shape
    own, width = stream.shape
    kr, units = gate_m.shape
    dc = down_m.shape[1]
    ring = n // 2
    side = (units // 128 - 1) // 2 * 128
    most = units - side
    group = 2 * tps * own
    dma = pltpu.SemaphoreType.DMA
    vmem = pl.BlockSpec(memory_space=pltpu.VMEM)
    hbm = pl.BlockSpec(memory_space=pl.ANY)
    count = 12 * ring
    arrays = (stream, qp, kp, vp, gp, strength, decay_pre, extra, rate[None, :], head_gain[None, :], feed_gain[None, :])
    return pl.pallas_call(
        functools.partial(paired_kernel, n, tps),
        out_shape=jax.ShapeDtypeStruct((own, width), BF16),
        in_specs=[hbm] * 15,
        out_specs=vmem,
        scratch_shapes=[
            *(pltpu.VMEM(a.shape, a.dtype) for a in arrays), dma((len(arrays),)),
            pltpu.VMEM((kr * n, units), BF16),
            pltpu.VMEM((kr * n, units), BF16),
            pltpu.VMEM((n,) + down_m.shape, BF16),
            pltpu.VMEM((tps,) + w_out.shape, BF16),
            pltpu.VMEM((heads, tokens, 2 * HEAD), F32),
            pltpu.VMEM((heads, HEAD, 2 * HEAD), BF16),
            pltpu.VMEM((heads, HEAD, 2 * HEAD), BF16),
            pltpu.VMEM((heads, HEAD, 2 * HEAD), BF16),
            pltpu.VMEM((heads, HEAD, HEAD), BF16),
            pltpu.VMEM((heads, HEAD, HEAD), BF16),
            pltpu.VMEM((heads, HEAD, HEAD), F32),
            pltpu.VMEM((tokens, heads * HEAD), BF16),
            pltpu.VMEM((tps - 1, own, heads * HEAD), BF16),
            pltpu.VMEM((own, width), F32),
            pltpu.VMEM((group, width), BF16),
            pltpu.VMEM((group, most), BF16),
            pltpu.VMEM((n, group, dc), F32),
            pltpu.VMEM((n, group // 2, dc), F32),
            pltpu.VMEM((n, group // 4, dc), F32),
            pltpu.VMEM((n, group // 2, dc), BF16),
            pltpu.VMEM((n, group // 2, dc), BF16),
            pltpu.VMEM((n, group // 4, dc), BF16),
            pltpu.VMEM((n, group // 4, dc), BF16),
            pltpu.VMEM((n, group // 8, dc), BF16),
            pltpu.VMEM((n, group // 8, dc), BF16),
            dma((count,)), dma((count,)), dma((10,)), dma((2,)), dma((2,)),
            dma((3,)), dma((3,)), dma((3,)), dma((3,)), dma((7,)), dma((7,)),
            dma((n,)), dma((n,)), dma((n,)), dma((n,)), dma((n,)), dma((n,)),
        ],
        compiler_params=pltpu.CompilerParams(
            collective_id=0, has_side_effects=True, vmem_limit_bytes=60 * 1024 * 1024),
    )(*arrays, w_out, gate_m, up_m, down_m)


def body(n, tps, *args):
    ring = n // 2
    short = ring % 4 == 0 and ring <= UNROLLED and tps == 4
    return (paired_body if short else chain_body)(n, tps, *args)


def solution(mesh):
    placed = (
        P(("sp", "tp"), None),
        P("sp", "tp"),
        P("sp", "tp"),
        P("sp", "tp"),
        P("sp", "tp"),
        P("tp", "sp"),
        P("tp", "sp"),
        P("tp", "sp"),
        P("tp"),
        P(),
        P("tp", None),
        P(),
        P("sp", "tp"),
        P("sp", "tp"),
        P("tp", "sp"),
    )
    return jax.shard_map(
        functools.partial(body, mesh.shape["sp"], mesh.shape["tp"]),
        mesh=mesh, in_specs=placed, out_specs=P(("sp", "tp"), None), check_vma=False,
    )
```

```python
import functools

import jax
import jax.numpy as jnp
from jax import lax
from jax.experimental import pallas as pl
from jax.experimental.pallas import tpu as pltpu
from jax.sharding import PartitionSpec as P

HEAD = 128
CHUNK = 128
UNROLLED = 4
EPSILON = 1e-06
F32 = jnp.float32
BF16 = jnp.bfloat16
HIGHEST = lax.Precision.HIGHEST
NN = (((1,), (0,)), ((), ()))
NT = (((1,), (1,)), ((), ()))
TN = (((0,), (0,)), ((), ()))


def dot1(a, b, dims=NN):
    return lax.dot_general(a, b, dims, preferred_element_type=F32)


def halves(x):
    high = x.astype(BF16)
    return high, (x - high.astype(F32)).astype(BF16)


def dot3(a, b, dims=NN):
    ah, al = halves(a)
    bh, bl = halves(b)
    return dot1(ah, bh, dims) + (dot1(ah, bl, dims) + dot1(al, bh, dims))


def silu(x):
    return x * jax.nn.sigmoid(x)


def local_scan(qp, kp, vp, strength, decay_pre, extra, rate, out_scr):
    heads, tokens = strength.shape
    chunks = tokens // CHUNK
    row_i = lax.broadcasted_iota(jnp.int32, (CHUNK, CHUNK), 0)
    col_i = lax.broadcasted_iota(jnp.int32, (CHUNK, CHUNK), 1)
    causal = row_i >= col_i
    strict = row_i > col_i
    eye = jnp.where(row_i == col_i, 1.0, 0.0).astype(F32)
    lower = jnp.where(causal, 1.0, 0.0).astype(F32)
    beta = jax.nn.sigmoid(strength[...].astype(F32))
    pre = decay_pre[...].astype(F32)
    soft = jnp.maximum(pre, 0.0) + jnp.log1p(jnp.exp(-jnp.abs(pre)))
    log_decay = -rate * soft + extra[...]

    pairs = [(h, c) for c in range(chunks) for h in range(heads)]
    data = {}
    for c in range(chunks):
        span = slice(c * CHUNK, (c + 1) * CHUNK)
        ld = log_decay[:, span]
        c_row = lax.dot_general(ld, lower, NT, precision=HIGHEST, preferred_element_type=F32)
        c_col = lax.dot_general(lower, ld, NT, precision=HIGHEST, preferred_element_type=F32)
        b_col = lax.dot_general(eye, beta[:, span], NT, precision=HIGHEST, preferred_element_type=F32)
        for h in range(heads):
            lanes = slice(h * HEAD, (h + 1) * HEAD)
            q = qp[span, lanes].astype(F32)
            k = kp[span, lanes].astype(F32)
            v = vp[span, lanes].astype(F32)
            q = q * (lax.rsqrt(jnp.sum(q * q, axis=-1, keepdims=True) + EPSILON) * HEAD ** (-0.5))
            k = k * lax.rsqrt(jnp.sum(k * k, axis=-1, keepdims=True) + EPSILON)
            cc = c_col[:, h:h + 1]
            bb = b_col[:, h:h + 1]
            cr = c_row[h:h + 1, :]
            last = cr[:, CHUNK - 1:]
            damp = jnp.where(causal, jnp.exp(jnp.where(causal, cc - cr, 0.0)), 0.0)
            grown = jnp.exp(cc)
            kb = k * bb
            kk = dot3(kb, k, NT) * jnp.where(strict, damp, 0.0)
            inner = dot3(q, k, NT) * damp
            data[h, c] = dict(
                low=kk, inner=inner, v=v * bb, kw=kb * grown, qd=q * grown,
                kd=k * jnp.exp(last - cc), decay=jnp.exp(last),
            )
    inverse = {}
    b = 1
    shift = 0
    while b < CHUNK:
        mask = ((row_i >> (shift + 1)) == (col_i >> (shift + 1))) & (
            ((row_i >> shift) & 1) == 1) & (((col_i >> shift) & 1) == 0)
        for key in pairs:
            piece = jnp.where(mask, data[key]["low"], 0.0)
            if b == 1:
                inverse[key] = eye - piece
            else:
                x = inverse[key]
                inverse[key] = x - dot3(x, dot3(piece, x))
        b *= 2
        shift += 1
    states = [jnp.concatenate([jnp.zeros((HEAD, HEAD), F32), eye], axis=1) for _ in range(heads)]
    for c in range(chunks):
        for h in range(heads):
            e = data[h, c]
            u = dot3(inverse[h, c], e["v"])
            w = dot3(inverse[h, c], e["kw"])
            x = states[h]
            new = jnp.concatenate([u, jnp.zeros_like(u)], axis=1) - dot3(w, x)
            out_scr[h, c * CHUNK:(c + 1) * CHUNK, :] = dot3(e["qd"], x) + dot3(e["inner"], new)
            states[h] = e["decay"] * x + dot3(e["kd"], new, TN)
    return states


def combine(states, x_part, p, p_send):
    heads = len(states)
    for h in range(heads):
        mine = states[h]
        theirs = x_part[h].astype(F32)
        before = jnp.where(p == 0, mine, theirs)
        after = jnp.where(p == 0, theirs, mine)
        after_s = jnp.concatenate([after[:, :HEAD], jnp.zeros((HEAD, HEAD), F32)], axis=1)
        p_send[h] = (dot3(after[:, HEAD:], before) + after_s).astype(BF16)


def fold_states(r, p_recv, s_in, heads):
    s_in[...] = jnp.zeros_like(s_in)

    def fold(i, _):
        for h in range(heads):
            got = p_recv[i, h].astype(F32)
            s_in[h] = dot3(got[:, HEAD:], s_in[h]) + got[:, :HEAD]
        return 0

    lax.fori_loop(0, r, fold, 0)


def apply_state(p, x_part, s_in, out_scr, head_gain, gp, mixed, heads):
    for h in range(heads):
        lanes = slice(h * HEAD, (h + 1) * HEAD)
        got = x_part[h].astype(F32)
        s = s_in[h]
        s = jnp.where(p == 0, s, dot3(got[:, HEAD:], s) + got[:, :HEAD])
        att = out_scr[h, :, :HEAD] + dot3(out_scr[h, :, HEAD:], s)
        att = att * lax.rsqrt(jnp.mean(att * att, axis=-1, keepdims=True) + EPSILON) * head_gain[...]
        mixed[:, lanes] = (att * silu(gp[:, lanes].astype(F32))).astype(BF16)


def messages(ring):
    own_z = [(a, 0, 0, way) for a in "GU" for way in "RL"]
    own_y = [(a, 0, 0, "Y") for a in "GU"]
    first = own_z + own_y
    down_y = [("D", 0, 0, "Y")]

    def relay(a, j, skip_y=False):
        out = []
        if j < ring - 1:
            out += [(a, -j, 0, "R"), (a, j, 0, "L")]
        if not skip_y:
            out += [(a, -j, 0, "Y"), (a, j, 0, "Y")]
        return out

    early, middle, later, last = [], [], [], []
    if ring > 1:
        early = relay("G", 1)
        middle = relay("U", 1)
        for j in range(2, ring):
            later += relay("G", j) + relay("U", j)
            if j == 2:
                later += [("D", 0, 0, "R"), ("D", 0, 0, "L")]
        if ring == 2:
            later += [("D", 0, 0, "R"), ("D", 0, 0, "L")]
        later += [("D", 0, 1, "R"), ("D", 0, 1, "L")]
        later += relay("D", 1, skip_y=True)
        for j in range(2, ring):
            last += relay("D", j)
    else:
        first = own_y
    return first, down_y, early, middle, later, last


def chain_kernel(
    n, tps, groups,
    stream, qp, kp, vp, gp, strength, decay_pre, extra, rate, head_gain, w_out, feed_gain,
    gate_in, up_in, down_in,
    result,
    gate_all, up_all, down_all, out_scr, x_send, x_part, p_send, p_recv, s_in, mixed,
    d_send, d_recv, residual, rows_all, hidden, f_part, f_recv,
    w_send, w_recv, own_sem, x_sem, p_ssem, p_rsem, d_ssem, d_rsem, e_ssem, e_rsem, f_ssem, f_rsem,
):
    ring = n // 2
    sp = lax.axis_index("sp")
    tp = lax.axis_index("tp")
    r = sp // 2
    p = lax.rem(sp, 2)
    heads = strength.shape[0]
    tokens = strength.shape[1]
    chunks = tokens // CHUNK
    own_rows = stream.shape[0]
    kr = gate_in.shape[0]
    MESH = pl.DeviceIdType.MESH

    def sp_of(dr, rel):
        q = p if rel == 0 else 1 - p
        return lax.rem(r + dr + ring, ring) * 2 + q

    partner = sp_of(0, 1)
    where = {"R": sp_of(1, 0), "L": sp_of(-1, 0), "Y": partner}

    def tp_peer(o):
        return lax.rem(tp + o, tps)

    barrier = pltpu.get_barrier_semaphore()
    for dr in range(1, ring):
        pl.semaphore_signal(barrier, 1, device_id=(sp_of(dr, 0), tp), device_id_type=MESH)
    pl.semaphore_signal(barrier, 1, device_id=(partner, tp), device_id_type=MESH)
    for o in range(1, tps):
        pl.semaphore_signal(barrier, 1, device_id=(sp, tp_peer(o)), device_id_type=MESH)
    pl.semaphore_wait(barrier, ring + tps - 1)

    flat = [m for g in groups for m in g]
    number = {m: i for i, m in enumerate(flat)}
    arrival = {}
    for (a, dr, rel, way) in flat:
        to = {"R": (dr - 1, rel), "L": (dr + 1, rel), "Y": (dr, 1 - rel)}[way]
        key = (a, to[0], to[1])
        assert key not in arrival
        arrival[key] = number[(a, dr, rel, way)]
    waited = set()
    copies = []

    def exists(dr):
        return (r + dr >= 0) & (r + dr < ring)

    def slot(a, dr, rel):
        s = sp_of(dr, rel)
        if a == "D":
            return down_all.at[s]
        whole = gate_all if a == "G" else up_all
        return whole.at[pl.ds(pl.multiple_of(s * kr, kr), kr), :]

    inputs = {"G": gate_in, "U": up_in, "D": down_in}

    def need(a, dr, rel):
        key = (a, dr, rel)
        if (dr == 0 and rel == 0) or key in waited:
            return
        waited.add(key)
        m = arrival[key]

        @pl.when(exists(dr))
        def _():
            here = slot(*key)
            pltpu.make_async_remote_copy(
                here, here, w_send.at[m], w_recv.at[m], device_id=(partner, tp), device_id_type=MESH
            ).wait_recv()

    def outgoing(message):
        a, dr, rel, way = message
        m = number[message]
        return pltpu.make_async_remote_copy(
            inputs[a] if dr == 0 and rel == 0 else slot(a, dr, rel),
            slot(a, dr, rel),
            w_send.at[m], w_recv.at[m],
            device_id=(where[way], tp), device_id_type=MESH,
        )

    def goes(message):
        ahead = {"R": r + 1 < ring, "L": r >= 1, "Y": r >= 0}[message[3]]
        return exists(message[1]) & ahead

    def pump(group):
        for message in group:
            need(*message[:3])

            @pl.when(goes(message))
            def _():
                outgoing(message).start()

            copies.append(message)

    def need_all(a):
        for dr in sorted(range(1 - ring, ring), key=abs):
            for rel in (0, 1):
                need(a, dr, rel)

    first, down_y, early, middle, later, last_group = groups
    pump(first)
    locals_ = []
    for i, a in enumerate("GUD"):
        local = pltpu.make_async_copy(inputs[a], slot(a, 0, 0), own_sem.at[i])
        local.start()
        locals_.append(local)

    states = local_scan(qp, kp, vp, strength, decay_pre, extra, rate[...], out_scr)
    for h in range(heads):
        x_send[h] = states[h].astype(BF16)
    x_copy = pltpu.make_async_remote_copy(
        x_send, x_part, x_sem.at[0], x_sem.at[1], device_id=(partner, tp), device_id_type=MESH)
    x_copy.start()
    pump(down_y)
    x_copy.wait_recv()
    combine(states, x_part, p, p_send)

    def p_copy(k, to, at):
        return pltpu.make_async_remote_copy(
            p_send, p_recv.at[at], p_ssem.at[k], p_rsem.at[k],
            device_id=(to, tp), device_id_type=MESH)

    for k in range(1, ring):
        @pl.when(r + k < ring)
        def _():
            p_copy(k, sp_of(k, 0), r).start()
    pump(early)
    for k in range(1, ring):
        @pl.when(r - k >= 0)
        def _():
            p_copy(k, sp_of(-k, 0), r - k).wait_recv()
    fold_states(r, p_recv, s_in, heads)
    apply_state(p, x_part, s_in, out_scr, head_gain, gp, mixed, heads)

    def rows_of(t):
        return pl.ds(pl.multiple_of(t * own_rows, own_rows), own_rows)

    order = [o for o in (2, 3, 1) if o < tps] + list(range(4, tps))
    d_copies = []
    for o in order:
        to = tp_peer(o)
        d_send[o - 1] = dot1(mixed[rows_of(to), :], w_out[...]).astype(BF16)
        copy = pltpu.make_async_remote_copy(
            d_send.at[o - 1], d_recv.at[o - 1], d_ssem.at[o - 1], d_rsem.at[o - 1],
            device_id=(sp, to), device_id_type=MESH)
        copy.start()
        d_copies.append(copy)
    pump(middle)
    total = dot1(mixed[rows_of(tp), :], w_out[...]).astype(BF16).astype(F32)
    for copy in d_copies:
        copy.wait_recv()
    for o in range(1, tps):
        total = total + d_recv[o - 1].astype(F32)
    total = stream[...].astype(F32) + total
    residual[...] = total
    rows_all[rows_of(tp), :] = (
        total * lax.rsqrt(jnp.mean(total * total, axis=-1, keepdims=True) + EPSILON) * feed_gain[...]
    ).astype(BF16)
    e_copies = []
    for o in order:
        copy = pltpu.make_async_remote_copy(
            rows_all.at[rows_of(tp), :], rows_all.at[rows_of(tp), :], e_ssem.at[o - 1], e_rsem.at[o - 1],
            device_id=(sp, tp_peer(o)), device_id_type=MESH)
        copy.start()
        e_copies.append(copy)
    for o in order:
        there = rows_all.at[rows_of(lax.rem(tp - o + tps, tps)), :]
        pltpu.make_async_remote_copy(
            there, there, e_ssem.at[o - 1], e_rsem.at[o - 1],
            device_id=(sp, tp_peer(o)), device_id_type=MESH).wait_recv()
    pump(later)
    need_all("G")
    need_all("U")
    for local in locals_:
        local.wait()

    tile = 128

    def ffn_in(i, _):
        lanes = pl.ds(pl.multiple_of(i * tile, tile), tile)
        both = dot1(rows_all[...], jnp.concatenate([gate_all[:, lanes], up_all[:, lanes]], axis=1))
        hidden[:, lanes] = (silu(both[:, :tile]) * both[:, tile:]).astype(BF16)
        return 0

    lax.fori_loop(0, gate_all.shape[1] // tile, ffn_in, 0)
    pump(last_group)
    need_all("D")
    dc = down_all.shape[2]
    pack = max(1, 128 // dc)
    wide = pack * dc

    def ffn_out(i, _):
        lanes = pl.ds(pl.multiple_of(i * wide, wide), wide)
        if pack == 1:
            weights = down_all[i]
        else:
            weights = jnp.concatenate([down_all[i * pack + j] for j in range(pack)], axis=1)
        f_part[:, lanes] = dot1(hidden[...], weights).astype(BF16)
        return 0

    lax.fori_loop(0, n // pack, ffn_out, 0)
    f_copies = []
    for o in order:
        copy = pltpu.make_async_remote_copy(
            f_part.at[rows_of(tp_peer(o)), :], f_recv.at[o - 1], f_ssem.at[o - 1], f_rsem.at[o - 1],
            device_id=(sp, tp_peer(o)), device_id_type=MESH)
        copy.start()
        f_copies.append(copy)
    ffn = f_part[rows_of(tp), :].astype(F32)
    for copy in f_copies:
        copy.wait_recv()
    for o in range(1, tps):
        ffn = ffn + f_recv[o - 1].astype(F32)
    result[...] = (residual[...] + ffn).astype(BF16)

    for message in copies:
        @pl.when(goes(message))
        def _():
            outgoing(message).wait_send()
    for copy in [x_copy] + d_copies + e_copies + f_copies:
        copy.wait_send()
    for k in range(1, ring):
        @pl.when(r + k < ring)
        def _():
            p_copy(k, sp_of(k, 0), r).wait_send()


def chain_body(n, tps, stream, qp, kp, vp, gp, strength, decay_pre, extra, rate, head_gain, w_out,
         feed_gain, gate_m, up_m, down_m):
    heads, tokens = strength.shape
    own, width = stream.shape
    kr, units = gate_m.shape
    ring = n // 2
    groups = messages(ring)
    count = sum(len(g) for g in groups)
    dma = pltpu.SemaphoreType.DMA
    vmem = pl.BlockSpec(memory_space=pltpu.VMEM)
    hbm = pl.BlockSpec(memory_space=pl.ANY)
    peers = max(1, tps - 1)
    return pl.pallas_call(
        functools.partial(chain_kernel, n, tps, groups),
        out_shape=jax.ShapeDtypeStruct((own, width), BF16),
        in_specs=[vmem] * 12 + [hbm] * 3,
        out_specs=vmem,
        scratch_shapes=[
            pltpu.VMEM((kr * n, units), BF16),
            pltpu.VMEM((kr * n, units), BF16),
            pltpu.VMEM((n,) + down_m.shape, BF16),
            pltpu.VMEM((heads, tokens, 2 * HEAD), F32),
            pltpu.VMEM((heads, HEAD, 2 * HEAD), BF16),
            pltpu.VMEM((heads, HEAD, 2 * HEAD), BF16),
            pltpu.VMEM((heads, HEAD, 2 * HEAD), BF16),
            pltpu.VMEM((ring, heads, HEAD, 2 * HEAD), BF16),
            pltpu.VMEM((heads, HEAD, HEAD), F32),
            pltpu.VMEM((tokens, heads * HEAD), BF16),
            pltpu.VMEM((peers, own, width), BF16),
            pltpu.VMEM((peers, own, width), BF16),
            pltpu.VMEM((own, width), F32),
            pltpu.VMEM((tokens, width), BF16),
            pltpu.VMEM((tokens, units), BF16),
            pltpu.VMEM((tokens, width), BF16),
            pltpu.VMEM((peers, own, width), BF16),
            dma((count,)), dma((count,)), dma((3,)), dma((2,)), dma((ring,)), dma((ring,)),
            dma((peers,)), dma((peers,)), dma((peers,)), dma((peers,)), dma((peers,)), dma((peers,)),
        ],
        compiler_params=pltpu.CompilerParams(
            collective_id=0, has_side_effects=True, vmem_limit_bytes=60 * 1024 * 1024),
    )(stream, qp, kp, vp, gp, strength, decay_pre, extra, rate[:, None], head_gain[None, :], w_out,
      feed_gain[None, :], gate_m, up_m, down_m)


def regions_of(ring, units):
    tiles = units // 128
    side = (tiles - 1) // 2 * 128
    half, quarter = ring // 2, ring // 4
    return {
        "L": (0, half, 0, side),
        "M": (quarter, half + quarter, side, units - side),
        "H": (half, ring, units - side, units),
    }


def paired_kernel(
    n, tps,
    stream_in, qp_in, kp_in, vp_in, gp_in, strength_in, decay_in, extra_in, rate_in, head_gain_in, feed_gain_in,
    w_out, gate_in, up_in, down_in,
    result,
    stream, qp, kp, vp, gp, strength, decay_pre, extra, rate, head_gain, feed_gain, in_sem,
    gate_all, up_all, down_all, w_all, out_scr, x_send, x_part, p_send, s_send, s_got, s_in, mixed, mix_all,
    residual, rows_all, hidden, acc, acc2, acc3, fd_send, fd_recv, fx_send, fx_recv, fz_send, fz_recv,
    w_send, w_recv, own_sem, x_sem, s_sem, wo_ssem, wo_rsem, m_ssem, m_rsem, t_ssem, t_rsem,
    fd_ssem, fd_rsem, fx_ssem, fx_rsem, fz_ssem, fz_rsem,
):
    loads = []
    for i, (src, dst) in enumerate((
        (strength_in, strength), (decay_in, decay_pre), (extra_in, extra), (rate_in, rate), (kp_in, kp), (qp_in, qp),
        (vp_in, vp), (gp_in, gp), (stream_in, stream), (head_gain_in, head_gain), (feed_gain_in, feed_gain),
    )):
        load = pltpu.make_async_copy(src, dst, in_sem.at[i])
        load.start()
        loads.append(load)
    ring = n // 2
    half = ring // 2
    sp = lax.axis_index("sp")
    tp = lax.axis_index("tp")
    r = sp // 2
    p = lax.rem(sp, 2)
    x = tp // 2
    c = lax.rem(tp, 2)
    zz = jnp.where(r >= half, 1, 0)
    heads = strength.shape[0]
    own_rows = stream.shape[0]
    kr, units = gate_in.shape
    width = stream.shape[1]
    dc = down_in.shape[1]
    MESH = pl.DeviceIdType.MESH
    regions = regions_of(ring, units)
    partner = r * 2 + 1 - p
    mate = lax.rem(r + half, ring) * 2 + p
    core = x * 2 + 1 - c
    across = (1 - x) * 2 + c
    diagonal = (1 - x) * 2 + 1 - c

    def at(q):
        return q * 2 + p

    def remote(src, dst, ssem, rsem, sp_to, tp_to):
        return pltpu.make_async_remote_copy(src, dst, ssem, rsem, device_id=(sp_to, tp_to), device_id_type=MESH)

    inputs = {"G": gate_in, "U": up_in, "D": down_in}
    def spans(g, k):
        return (k >= regions[g][0]) & (k < regions[g][1])

    taken = {"send": [], "recv": []}

    def color(kind, users):
        for i, held in enumerate(taken[kind]):
            if not held & users:
                held |= users
                return i
        taken[kind].append(set(users))
        return len(taken[kind]) - 1

    number = {}
    for a in "GUD":
        for g in "LMH":
            for q in range(ring):
                for rel in (0, 1):
                    users = {k for k in range(ring) if spans(g, k) and (rel == 1 or k != q)}
                    number[a, g, q, rel] = color("recv", users)

    def slot(a, g, q, rel):
        s = q * 2 + (p if rel == 0 else 1 - p)
        c0, c1 = regions[g][2:]
        if a == "D":
            return down_all.at[s, c0:c1, :]
        whole = gate_all if a == "G" else up_all
        return whole.at[pl.ds(pl.multiple_of(s * kr, kr), kr), c0:c1]

    def own(a, g):
        c0, c1 = regions[g][2:]
        return inputs[a].at[c0:c1, :] if a == "D" else inputs[a].at[:, c0:c1]

    def member(g):
        return spans(g, r)

    own_copies = []
    for i, a in enumerate("GUD"):
        for j, g in enumerate("LMH"):
            for q in range(*regions[g][:2]):
                copy = pltpu.make_async_copy(own(a, g), slot(a, g, q, 0), own_sem.at[3 * i + j])
                own_copies.append((r == q, copy))

                @pl.when(r == q)
                def _():
                    copy.start()

    w_local = pltpu.make_async_copy(w_out, w_all.at[tp], own_sem.at[9])
    w_local.start()

    barrier = pltpu.get_barrier_semaphore()
    for k in range(1, ring):
        pl.semaphore_signal(barrier, 1, device_id=(at(lax.rem(r + k, ring)), tp), device_id_type=MESH)
    pl.semaphore_signal(barrier, 1, device_id=(partner, tp), device_id_type=MESH)
    for k in range(1, tps):
        pl.semaphore_signal(barrier, 1, device_id=(sp, lax.rem(tp + k, tps)), device_id_type=MESH)
    pl.semaphore_wait(barrier, ring + tps - 1)

    def detour(a, g, q, to):
        lo, hi = regions[g][:2]
        if g == "M" or hi - lo < 2:
            return False
        inner, outer = (hi - 1, hi - 2) if g == "L" else (lo, lo + 1)
        return a != "G" and (q, to) == (outer, inner)

    sends = []
    waited = set()

    def send(cond, src, key, way, sp_to):
        users = {k for k in range(ring) if cond(k)}
        if not users:
            return
        m = color("send", users)
        landing = key[:3] + (1,) if way == "y" else key

        def make():
            return remote(src, slot(*key), w_send.at[m], w_recv.at[number[landing]], sp_to, tp)

        @pl.when(cond(r))
        def _():
            make().start()

        sends.append((cond(r), make))

    def forwards_y(a, g, q, k):
        return spans(g, k) and not detour(a, g, q, k)

    def own_sends(a, ways, only=None):
        for g in "LMH":
            lo, hi = regions[g][:2]
            for q in range(ring):
                if only is not None and q not in only:
                    continue
                key = (a, g, q, 0)
                mine = functools.partial(lambda q, k: k == q, q)
                inside = lo <= q < hi
                here = slot(*key) if inside else own(a, g)
                if inside and "y" in ways:
                    send(mine, here, key, "y", partner)
                if g == "M":
                    targets = [to for to in range(lo, hi) if to != q]
                elif inside:
                    targets = [to for to in (q - 1, q + 1) if lo <= to < hi]
                else:
                    targets = [lo if q < lo else hi - 1]
                for to in targets:
                    way = "l" if to < q else "r"
                    if (way if abs(q - to) == 1 else way.upper()) in ways:
                        send(mine, here, key, way, at(to))

    def arrived(key, cond):
        here = slot(*key)

        @pl.when(cond)
        def _():
            remote(here, here, w_send.at[0], w_recv.at[number[key]], partner, tp).wait_recv()

    def role_of(g, role, k):
        lo, hi = regions[g][:2]
        inner = hi - 1 if g == "L" else lo
        return True if role is None else (k == inner) if role == "in" else (k != inner)

    def relay(a, g, q, role):
        key = (a, g, q, 0)
        lo, hi = regions[g][:2]
        assert (key, role) not in waited
        waited.add((key, role))

        def holds(k):
            return spans(g, k) & (k != q) & role_of(g, role, k)

        if any(holds(k) for k in range(ring)):
            arrived(key, holds(r))
        here = slot(*key)
        if g != "M":
            send(lambda k: holds(k) & (k > lo) & (k < q), here, key, "l", at(r - 1))
            send(lambda k: holds(k) & (k > q) & (k < hi - 1), here, key, "r", at(r + 1))
        for k in range(lo, hi):
            if holds(k) and forwards_y(a, g, q, k):
                send(functools.partial(lambda k, kk: kk == k, k), here, key, "y", partner)

    def detours(a):
        for g in "LH":
            for q in range(*regions[g][:2]):
                for to in (q - 1, q + 1):
                    if detour(a, g, q, to):
                        key = (a, g, q, 1)
                        arrived(key, r == q)
                        early.setdefault(key, []).append(q)
                        send(functools.partial(lambda q, k: k == q, q), slot(*key), key, "z", at(to))

    early = {}
    low = list(range(half - 1, -1, -1)) + list(range(half, ring))

    def relays(a, role, g, *steps):
        for i in steps:
            relay(a, g, low[i] if g == "L" else ring - 1 - low[i], role)

    def middles(a):
        for q in range(ring):
            relay(a, "M", q, None)

    def finish(a, q, rel):
        for g in "LMH":
            key = (a, g, q, rel)
            if rel == 1:
                cond = member(g)
                for done in early.get(key, []):
                    cond = cond & (r != done)
                arrived(key, cond)
                continue
            for role in (None,) if g == "M" else ("in", "out"):
                if (key, role) not in waited:
                    waited.add((key, role))
                    mine = member(g) & (r != q)
                    arrived(key, mine & role_of(g, role, r))

    for cond, copy in own_copies:
        @pl.when(cond)
        def _():
            copy.wait()
    own_sends("G", "LR")
    own_sends("G", "ly")
    own_sends("G", "r", range(1, ring))
    w_local.wait()
    w_x = remote(w_all.at[tp], w_all.at[tp], wo_ssem.at[0], wo_rsem.at[0], sp, across)
    w_half = w_out.shape[0] // 2
    w_part = w_all.at[tp, :w_half, :]
    remote(w_part, w_part, wo_ssem.at[0], wo_rsem.at[0], sp, across).start()
    w_d = remote(w_all.at[tp], w_all.at[tp], wo_ssem.at[1], wo_rsem.at[1], sp, core)
    w_d.start()
    w_xd = remote(w_all.at[across], w_all.at[across], wo_ssem.at[2], wo_rsem.at[2], sp, core)

    for load in loads:
        load.wait()
    square = (heads, heads)
    same = lax.broadcasted_iota(jnp.int32, square, 0) == lax.broadcasted_iota(jnp.int32, square, 1)
    rates = jnp.sum(jnp.where(same, jnp.broadcast_to(rate[...], square), 0.0), axis=1, keepdims=True)
    states = local_scan(qp, kp, vp, strength, decay_pre, extra, rates, out_scr)
    for h in range(heads):
        x_send[h] = states[h].astype(BF16)
    x_copy = remote(x_send, x_part, x_sem.at[0], x_sem.at[1], partner, tp)
    x_copy.start()
    own_sends("U", "lL")
    own_sends("U", "r", range(half, ring))
    x_copy.wait_recv()
    combine(states, x_part, p, p_send)

    def s_copy(src, to):
        return remote(src, s_got, s_sem.at[0], s_sem.at[1], at(to), tp)

    s_in[...] = jnp.zeros_like(s_in)

    @pl.when(r == 0)
    def _():
        s_copy(p_send.at[:, :, :HEAD], 1).start()

    own_sends("G", "r", range(1))
    w_rest = w_all.at[tp, w_half:, :]
    remote(w_rest, w_rest, wo_ssem.at[0], wo_rsem.at[0], sp, across).start()
    own_sends("U", "y")
    relays("G", "out", "L", 0)
    relays("G", "out", "H", 0)
    relays("G", "in", "H", 1)

    @pl.when(r > 0)
    def _():
        s_copy(s_send, 0).wait_recv()
        for h in range(heads):
            s_in[h] = s_got[h].astype(F32)

    @pl.when((r > 0) & (r + 1 < ring))
    def _():
        for h in range(heads):
            both = p_send[h].astype(F32)
            s_send[h] = (dot3(both[:, HEAD:], s_in[h]) + both[:, :HEAD]).astype(BF16)
        s_copy(s_send, lax.rem(r + 1, ring)).start()

    own_sends("U", "r", range(1, half))
    relays("G", "in", "L", 2, 3)
    own_sends("D", "y", [q for q in range(ring) if q not in (half - 1, half)])
    w_x.wait_recv()
    w_xd.start()
    own_sends("U", "R")
    apply_state(p, x_part, s_in, out_scr, head_gain, gp, mixed, heads)

    def token_rows(t):
        return pl.ds(pl.multiple_of(t * own_rows, own_rows), own_rows)

    mix_copies = []
    for i, to in enumerate((across, diagonal, core)):
        copy = remote(mixed.at[token_rows(to), :], mix_all.at[i], m_ssem.at[i], m_rsem.at[i], sp, to)
        copy.start()
        mix_copies.append((to, copy))
    relays("G", "in", "H", 2, 3)
    relays("G", "in", "L", 1)
    relays("G", "out", "L", 2)
    relays("U", "out", "L", 0)
    total = dot1(mixed[token_rows(tp), :], w_all[tp]).astype(BF16).astype(F32)
    w_d.wait_recv()
    w_xd.wait_recv()
    for i, (to, copy) in enumerate(mix_copies):
        copy.wait_recv()
        total = total + dot1(mix_all[i], w_all[to]).astype(BF16).astype(F32)
    total = stream[...].astype(F32) + total
    residual[...] = total
    normed = (
        total * lax.rsqrt(jnp.mean(total * total, axis=-1, keepdims=True) + EPSILON) * feed_gain[...]
    ).astype(BF16)

    def block_of(z_, x_, c_):
        b = (c_ * 2 + x_) * 2 + z_
        return rows_all.at[pl.ds(pl.multiple_of(b * own_rows, own_rows), own_rows), :]

    b_own = (c * 2 + x) * 2 + zz
    rows_all[pl.ds(pl.multiple_of(b_own * own_rows, own_rows), own_rows), :] = normed
    t_copies = []

    def token(i, block, sp_to, tp_to):
        copy = remote(block, block, t_ssem.at[i], t_rsem.at[i], sp_to, tp_to)
        copy.start()
        t_copies.append(copy)

    def token_wait(i, block):
        remote(block, block, t_ssem.at[i], t_rsem.at[i], sp, across).wait_recv()

    token(0, block_of(zz, x, c), mate, tp)
    token(1, block_of(zz, x, c), sp, across)
    token(2, block_of(zz, x, c), sp, core)
    own_sends("U", "r", range(1))
    relays("G", "out", "L", 3)
    relays("G", "out", "H", 2)
    relays("U", "in", "L", 2)
    relays("U", "out", "H", 0)
    middles("G")
    detours("U")
    relays("U", "in", "L", 3)
    token_wait(1, block_of(zz, 1 - x, c))
    token(5, block_of(zz, 1 - x, c), sp, core)
    relays("G", "out", "H", 3)
    relays("U", "in", "H", 2, 3)
    own_sends("D", "lr")
    relays("U", "out", "L", 2)
    relays("U", "out", "H", 2)
    own_sends("D", "LR")
    token_wait(0, block_of(1 - zz, x, c))
    token(3, block_of(1 - zz, x, c), sp, across)
    token(4, block_of(1 - zz, x, c), sp, core)
    relays("U", "out", "L", 3)
    relays("U", "out", "H", 3)
    middles("U")
    own_sends("D", "y", (half - 1, half))
    token_wait(3, block_of(1 - zz, 1 - x, c))
    token(6, block_of(1 - zz, 1 - x, c), sp, core)
    relays("D", "out", "L", 0)
    relays("D", "out", "H", 0)
    relays("D", "in", "L", 2)
    detours("D")
    relays("D", "in", "H", 2)
    relays("D", "in", "L", 3)
    token_wait(2, block_of(zz, x, 1 - c))
    token_wait(4, block_of(1 - zz, x, 1 - c))
    token_wait(5, block_of(zz, 1 - x, 1 - c))
    token_wait(6, block_of(1 - zz, 1 - x, 1 - c))
    for a in "GU":
        for rel in (0, 1):
            for q in range(ring):
                finish(a, q, rel)

    has_m = member("M")
    first = jnp.where(r < half, 0, jnp.where(has_m, regions["M"][2] // 128, regions["H"][2] // 128))
    many = (regions["L"][3] - regions["L"][2]) // 128 + jnp.where(has_m, (regions["M"][3] - regions["M"][2]) // 128, 0)

    def ffn_in(i, _):
        lanes = pl.ds(pl.multiple_of((first + i) * 128, 128), 128)
        both = dot1(rows_all[...], jnp.concatenate([gate_all[:, lanes], up_all[:, lanes]], axis=1))
        hidden[:, pl.ds(pl.multiple_of(i * 128, 128), 128)] = (silu(both[:, :128]) * both[:, 128:]).astype(BF16)
        return 0

    lax.fori_loop(0, many, ffn_in, 0)
    inner, outer = list(range(half, half - 2, -1)), [q for q in range(ring - 1, -1, -1) if q not in (half - 1, half)]
    order = [(q, 0) for q in inner + outer[:1]] + [(inner[0], 1)] + [(q, 0) for q in outer[1:]]
    order += [(q, 1) for q in inner[1:] + outer]
    side = regions["L"][3]
    mids = regions["M"][3] - regions["M"][2]
    base = pl.multiple_of(first * 128, 128)
    f_sends = []

    def lanes_of(i):
        q, rel = order[i]
        s = q * 2 + (p if rel == 0 else 1 - p)
        return s, pl.ds(pl.multiple_of(s * dc, dc), dc)

    hop = 4 * own_rows

    def stage_a(i):
        q, rel = order[i]
        finish("D", q, rel)
        s, _ = lanes_of(i)

        @pl.when(has_m)
        def _():
            acc[i] = dot1(hidden[...], down_all[s, pl.ds(base, side + mids), :])

        @pl.when(jnp.logical_not(has_m))
        def _():
            acc[i] = dot1(hidden[:, :side], down_all[s, pl.ds(base, side), :])

        fd_send[i] = acc[i, pl.ds(pl.multiple_of((1 - c) * hop, hop), hop), :].astype(BF16)
        copy = remote(fd_send.at[i], fd_recv.at[i], fd_ssem.at[i], fd_rsem.at[i], sp, core)
        copy.start()
        f_sends.append(copy)

    def stage_b(i):
        f = remote(fd_send.at[i], fd_recv.at[i], fd_ssem.at[i], fd_rsem.at[i], sp, core)
        f.wait_recv()
        acc2[i] = acc[i, pl.ds(pl.multiple_of(c * hop, hop), hop), :] + fd_recv[i].astype(F32)
        fx_send[i] = acc2[i, pl.ds(pl.multiple_of((1 - x) * (hop // 2), hop // 2), hop // 2), :].astype(BF16)
        copy = remote(fx_send.at[i], fx_recv.at[i], fx_ssem.at[i], fx_rsem.at[i], sp, across)
        copy.start()
        f_sends.append(copy)

    def stage_c(i):
        f = remote(fx_send.at[i], fx_recv.at[i], fx_ssem.at[i], fx_rsem.at[i], sp, across)
        f.wait_recv()
        acc3[i] = acc2[i, pl.ds(pl.multiple_of(x * (hop // 2), hop // 2), hop // 2), :] + fx_recv[i].astype(F32)
        fz_send[i] = acc3[i, pl.ds(pl.multiple_of((1 - zz) * own_rows, own_rows), own_rows), :].astype(BF16)
        copy = remote(fz_send.at[i], fz_recv.at[i], fz_ssem.at[i], fz_rsem.at[i], mate, tp)
        copy.start()
        f_sends.append(copy)

    def stage_d(i):
        f = remote(fz_send.at[i], fz_recv.at[i], fz_ssem.at[i], fz_rsem.at[i], mate, tp)
        f.wait_recv()
        _, lanes = lanes_of(i)
        ffn = acc3[i, pl.ds(pl.multiple_of(zz * own_rows, own_rows), own_rows), :] + fz_recv[i].astype(F32)
        result[:, lanes] = (residual[:, lanes] + ffn).astype(BF16)

    ahead = {
        0: (("in", "H", 3), ("out", "L", 2)),
        1: (("out", "H", 2),),
        2: (("out", "L", 3),),
        4: (("out", "H", 3),),
    }
    for i in range(n + 5):
        for role, g, step in ahead.get(i, ()):
            relays("D", role, g, step)
        if i == 0:
            middles("D")
        if i < n:
            stage_a(i)
        if 0 <= i - 1 < n:
            stage_b(i - 1)
        if 0 <= i - 3 < n:
            stage_c(i - 3)
        if 0 <= i - 5 < n:
            stage_d(i - 5)

    for cond, make in sends:
        @pl.when(cond)
        def _():
            make().wait_send()
    for copy in [x_copy, w_x, w_d, w_xd] + [m for _, m in mix_copies] + t_copies + f_sends:
        copy.wait_send()

    @pl.when(r == 0)
    def _():
        s_copy(p_send.at[:, :, :HEAD], 1).wait_send()

    @pl.when((r > 0) & (r + 1 < ring))
    def _():
        s_copy(s_send, 0).wait_send()

    assert max(len(taken["send"]), len(taken["recv"])) <= w_send.shape[0]


def paired_body(n, tps, stream, qp, kp, vp, gp, strength, decay_pre, extra, rate, head_gain, w_out,
                feed_gain, gate_m, up_m, down_m):
    heads, tokens = strength.shape
    own, width = stream.shape
    kr, units = gate_m.shape
    dc = down_m.shape[1]
    ring = n // 2
    side = (units // 128 - 1) // 2 * 128
    most = units - side
    group = 2 * tps * own
    dma = pltpu.SemaphoreType.DMA
    vmem = pl.BlockSpec(memory_space=pltpu.VMEM)
    hbm = pl.BlockSpec(memory_space=pl.ANY)
    count = 12 * ring
    arrays = (stream, qp, kp, vp, gp, strength, decay_pre, extra, rate[None, :], head_gain[None, :], feed_gain[None, :])
    return pl.pallas_call(
        functools.partial(paired_kernel, n, tps),
        out_shape=jax.ShapeDtypeStruct((own, width), BF16),
        in_specs=[hbm] * 15,
        out_specs=vmem,
        scratch_shapes=[
            *(pltpu.VMEM(a.shape, a.dtype) for a in arrays), dma((len(arrays),)),
            pltpu.VMEM((kr * n, units), BF16),
            pltpu.VMEM((kr * n, units), BF16),
            pltpu.VMEM((n,) + down_m.shape, BF16),
            pltpu.VMEM((tps,) + w_out.shape, BF16),
            pltpu.VMEM((heads, tokens, 2 * HEAD), F32),
            pltpu.VMEM((heads, HEAD, 2 * HEAD), BF16),
            pltpu.VMEM((heads, HEAD, 2 * HEAD), BF16),
            pltpu.VMEM((heads, HEAD, 2 * HEAD), BF16),
            pltpu.VMEM((heads, HEAD, HEAD), BF16),
            pltpu.VMEM((heads, HEAD, HEAD), BF16),
            pltpu.VMEM((heads, HEAD, HEAD), F32),
            pltpu.VMEM((tokens, heads * HEAD), BF16),
            pltpu.VMEM((tps - 1, own, heads * HEAD), BF16),
            pltpu.VMEM((own, width), F32),
            pltpu.VMEM((group, width), BF16),
            pltpu.VMEM((group, most), BF16),
            pltpu.VMEM((n, group, dc), F32),
            pltpu.VMEM((n, group // 2, dc), F32),
            pltpu.VMEM((n, group // 4, dc), F32),
            pltpu.VMEM((n, group // 2, dc), BF16),
            pltpu.VMEM((n, group // 2, dc), BF16),
            pltpu.VMEM((n, group // 4, dc), BF16),
            pltpu.VMEM((n, group // 4, dc), BF16),
            pltpu.VMEM((n, group // 8, dc), BF16),
            pltpu.VMEM((n, group // 8, dc), BF16),
            dma((count,)), dma((count,)), dma((10,)), dma((2,)), dma((2,)),
            dma((3,)), dma((3,)), dma((3,)), dma((3,)), dma((7,)), dma((7,)),
            dma((n,)), dma((n,)), dma((n,)), dma((n,)), dma((n,)), dma((n,)),
        ],
        compiler_params=pltpu.CompilerParams(
            collective_id=0, has_side_effects=True, vmem_limit_bytes=60 * 1024 * 1024),
    )(*arrays, w_out, gate_m, up_m, down_m)


def body(n, tps, *args):
    ring = n // 2
    short = ring % 4 == 0 and ring <= UNROLLED and tps == 4
    return (paired_body if short else chain_body)(n, tps, *args)


def solution(mesh):
    placed = (
        P(("sp", "tp"), None),
        P("sp", "tp"),
        P("sp", "tp"),
        P("sp", "tp"),
        P("sp", "tp"),
        P("tp", "sp"),
        P("tp", "sp"),
        P("tp", "sp"),
        P("tp"),
        P(),
        P("tp", None),
        P(),
        P("sp", "tp"),
        P("sp", "tp"),
        P("tp", "sp"),
    )
    return jax.shard_map(
        functools.partial(body, mesh.shape["sp"], mesh.shape["tp"]),
        mesh=mesh, in_specs=placed, out_specs=P(("sp", "tp"), None), check_vma=False,
    )
```
